32 devices in a mesh: sp: 8 (over z, x), tp: 4 (over y, core).
Axes of the slice: x: 2, y: 2, z: 4, core: 2. Of those that a mesh axis runs over, the one named last changes fastest.
Arguments:
- query_wide: bfloat16 [6144, 8, 256], P('sp', 'tp'), may hold values from -6 to 6
- key_wide: bfloat16 [6144, 8, 256], P('sp', 'tp'), may hold values from -6 to 6
- value_wide: bfloat16 [6144, 8, 256], P('sp', 'tp'), may hold values from -6 to 6
- query_narrow: bfloat16 [6144, 8, 128], P('sp', 'tp'), may hold values from -6 to 6
- key_narrow: bfloat16 [6144, 8, 128], P('sp', 'tp'), may hold values from -6 to 6
- value_narrow: bfloat16 [6144, 8, 128], P('sp', 'tp'), may hold values from -6 to 6
- mix_lambda: float32 [2, 8], P(None, 'tp'), may hold values from 0.3 to 0.8
- residual_in: bfloat16 [6144, 2048], P(('sp', 'tp')), may hold values from -6 to 6
- out_wide: bfloat16 [2048, 2048], P('tp'), may hold values from -0.109375 to 0.109375
- out_narrow: bfloat16 [1024, 2048], P('tp'), may hold values from -0.109375 to 0.109375
- ffn_gain: float32 [2048], replicated, may hold values from 0.1 to 1.9
- expert_ids: int32 [6144, 2], P(('sp', 'tp')), may hold values from 0 to 31, as said below
- expert_weights: float32 [6144, 2], P(('sp', 'tp')), may hold values from 0.1 to 1
- gate_weight: bfloat16 [32, 2048, 1024], P(('sp', 'tp')), may hold values from -0.125 to 0.125
- up_weight: bfloat16 [32, 2048, 1024], P(('sp', 'tp')), may hold values from -0.125 to 0.125
- down_weight: bfloat16 [32, 1024, 2048], P(('sp', 'tp')), may hold values from -0.1875 to 0.1875
Outputs:
- layer_out: bfloat16 [6144, 2048], P(('sp', 'tp'))
The draws below stay inside these ranges and needn't reach their ends.
Inputs may be any that keep to these rules, and one draw needn't show every extreme that they name: `expert_ids`: A row's two experts differ and lie in the same group of 4 consecutive experts (8 groups). In each aligned block of 192 rows (the rows of one device) no expert is named by more than 24 rows, and in every block some expert is named by exactly 24 rows.
All inputs are finite; a program needn't handle non-finite values.
Results may differ from the reference program's by a relative error of at most 0.015.
Values may be sent and summed in bfloat16 or wider, within the bound.
A program may use at most 192 MiB of HBM per device.

```python
import math
import jax
import jax.numpy as jnp
from jax import lax

D = 2048
HEADS = 8
DA = 128
DB = 64
VA = 256
VB = 128
FF = 1024
GROUP_SIZE = 4
TOKENS = 6144
TOK_LOC = 192
EXPERTS = 32
CAP = 24


def query_draw(key, salt, head_size):
    values_drawn = jnp.clip(jax.random.normal(jax.random.fold_in(key, salt + 100), (TOKENS, HEADS, 2 * head_size), jnp.float32) * 1.3, -6.0, 6.0)
    return values_drawn.astype(jnp.bfloat16)


def key_draw(key, salt, head_size):
    values_drawn = jnp.clip(jax.random.normal(jax.random.fold_in(key, salt + 200), (TOKENS, HEADS, 2 * head_size), jnp.float32) * 1.3, -6.0, 6.0)
    return values_drawn.astype(jnp.bfloat16)


def draw_query_wide(key, part):
    return query_draw(key, 5, DA)


def draw_key_wide(key, part):
    return key_draw(key, 5, DA)


def draw_query_narrow(key, part):
    return query_draw(key, 9, DB)


def draw_key_narrow(key, part):
    return key_draw(key, 9, DB)


def draw_expert_ids(key, part):
    positions = EXPERTS * CAP // 2
    blocks = TOKENS // TOK_LOC
    forced = jax.random.randint(jax.random.fold_in(key, 31), (), 0, EXPERTS)
    pair_first = jnp.array([[0, 2], [0, 1], [0, 1]], jnp.int32)
    pair_second = jnp.array([[1, 3], [2, 3], [3, 2]], jnp.int32)

    def one_block(block_key):
        key_kind, key_score, key_order, key_flip = jax.random.split(block_key, 4)
        position = jnp.arange(positions, dtype=jnp.int32)
        group_index = position // (2 * CAP)
        level_index = position % (2 * CAP) // 2
        which_pair = position % 2
        pair_kind = jax.random.randint(key_kind, (EXPERTS // GROUP_SIZE, CAP), 0, 3)
        kinds = pair_kind[group_index, level_index]
        first_expert = pair_first[kinds, which_pair] + group_index * GROUP_SIZE
        second_expert = pair_second[kinds, which_pair] + group_index * GROUP_SIZE
        hit = ((first_expert == forced) | (second_expert == forced)).astype(jnp.int32)
        priority = jax.random.randint(key_score, (positions,), 0, 2 ** 20) * 1024 + position + hit * 2 ** 30
        _, chosen = lax.top_k(priority, TOK_LOC)
        shuffle = jax.random.permutation(key_order, TOK_LOC)
        picked = chosen[shuffle]
        flipped = jax.random.randint(key_flip, (TOK_LOC,), 0, 2)
        left_expert = first_expert[picked]
        right_expert = second_expert[picked]
        low_expert = jnp.where(flipped == 1, right_expert, left_expert)
        high_expert = jnp.where(flipped == 1, left_expert, right_expert)
        return jnp.stack([low_expert, high_expert], axis=-1)
    block_keys = jax.random.split(jax.random.fold_in(key, 32), blocks)
    return jax.vmap(one_block)(block_keys).reshape(TOKENS, 2).astype(jnp.int32)


def steps_of(stream_key, dims, cuts, smallest, top_value):
    gain, own = 1.0, jax.random.fold_in(stream_key, 6)
    for dim, shards_of in cuts:
        steps = jnp.exp(jax.random.uniform(jax.random.fold_in(own, dim), (shards_of,), jnp.float32, smallest / len(cuts), top_value / len(cuts)))
        gain = gain * jnp.repeat(steps, dims[dim] // shards_of).reshape([-1 if axis == dim else 1 for axis in range(len(dims))])
    return gain


def centred(stream_key, dims, spread, reach, pieces=(), kind=jnp.bfloat16):
    values = spread * jax.random.normal(stream_key, dims, jnp.float32)
    if pieces:
        values = values * steps_of(stream_key, dims, pieces, -0.22, 0.18)
    return jnp.clip(values, -reach, reach).astype(kind)


def setup_inputs(seed: int = 0) -> dict:
    streams_of = jax.random.split(jax.random.key(seed), 17)
    return {
        "query_wide": draw_query_wide(jax.random.fold_in(streams_of[16], 71), 0),
        "key_wide": draw_key_wide(jax.random.fold_in(streams_of[16], 71), 0),
        "value_wide": centred(streams_of[2], (TOKENS, HEADS, VA), 1.0, 6.0, ((0, 8), (1, 4))),
        "query_narrow": draw_query_narrow(jax.random.fold_in(streams_of[16], 71), 0),
        "key_narrow": draw_key_narrow(jax.random.fold_in(streams_of[16], 71), 0),
        "value_narrow": centred(streams_of[5], (TOKENS, HEADS, VB), 1.0, 6.0, ((0, 8), (1, 4))),
        "mix_lambda": jnp.clip(0.3 + 0.5 * jax.random.uniform(streams_of[6], (2, HEADS), jnp.float32) ** steps_of(streams_of[6], (2, HEADS), ((1, 4),), -0.2, 0.2), 0.3, 0.8),
        "residual_in": centred(streams_of[7], (TOKENS, D), 1.0, 6.0, ((0, 32),)),
        "out_wide": centred(streams_of[8], (HEADS * VA, D), (HEADS * VA + HEADS * VB) ** -0.5, 0.109375, ((0, 4),)),
        "out_narrow": centred(streams_of[9], (HEADS * VB, D), (HEADS * VA + HEADS * VB) ** -0.5, 0.109375, ((0, 4),)),
        "ffn_gain": jnp.clip(1.0 + 0.18 * jax.random.normal(streams_of[10], (D,), jnp.float32), 0.1, 1.9),
        "expert_ids": draw_expert_ids(jax.random.fold_in(streams_of[16], 71), 0),
        "expert_weights": jnp.clip(0.1 + 0.9 * jax.random.uniform(streams_of[12], (TOKENS, 2), jnp.float32) ** steps_of(streams_of[12], (TOKENS, 2), ((0, 32),), -0.2, 0.2), 0.1, 1.0),
        "gate_weight": centred(streams_of[13], (EXPERTS, D, FF), D ** -0.5, 0.125, ((0, 32),)),
        "up_weight": centred(streams_of[14], (EXPERTS, D, FF), D ** -0.5, 0.125, ((0, 32),)),
        "down_weight": centred(streams_of[15], (EXPERTS, FF, D), FF ** -0.5, 0.1875, ((0, 32),)),
    }


def head_group(query, keys, values, lam_row, head_size):
    score_scale = head_size ** (-0.5)
    query_block = math.gcd(TOKENS, 512)
    query_f = query.astype(jnp.float32)
    keys_f = keys.astype(jnp.float32)
    values_f = values.astype(jnp.float32)
    key_pos = jnp.arange(TOKENS, dtype=jnp.int32)

    def block_read(number):
        query_rows = lax.dynamic_slice_in_dim(query_f, number * query_block, query_block, 0)
        query_pos = number * query_block + jnp.arange(query_block, dtype=jnp.int32)
        causal = key_pos[None, :] <= query_pos[:, None]
        reads = []
        for which_map in range(2):
            lower_edge = which_map * head_size
            scores = jnp.einsum('qhd,khd->hqk', query_rows[..., lower_edge:lower_edge + head_size], keys_f[..., lower_edge:lower_edge + head_size]) * score_scale
            scores = jnp.where(causal[None], scores, -jnp.inf)
            new_peak = lax.optimization_barrier(jnp.max(scores, axis=-1, keepdims=True))
            expo = jnp.exp(scores - new_peak)
            totals = lax.optimization_barrier(jnp.sum(expo, axis=-1))
            rounded = lax.optimization_barrier(expo.astype(jnp.bfloat16)).astype(jnp.float32)
            reads.append(jnp.einsum('hqk,khv->hqv', rounded, values_f) / totals[..., None])
        mixed_read = reads[0] - lam_row[:, None, None] * reads[1]
        normed = mixed_read * lax.rsqrt(lax.optimization_barrier(jnp.mean(mixed_read * mixed_read, axis=-1, keepdims=True)) + 1e-06)
        return jnp.transpose(normed.astype(jnp.bfloat16), (1, 0, 2))
    outputs = lax.map(block_read, jnp.arange(TOKENS // query_block, dtype=jnp.int32))
    return outputs.reshape(TOKENS, -1)

def reference(query_wide, key_wide, value_wide, query_narrow, key_narrow, value_narrow, mix_lambda, residual_in, out_wide, out_narrow, ffn_gain, expert_ids, expert_weights, gate_weight, up_weight, down_weight):
    heads_wide = head_group(query_wide, key_wide, value_wide, mix_lambda[0], DA)
    heads_narrow = head_group(query_narrow, key_narrow, value_narrow, mix_lambda[1], DB)
    projected = jnp.dot(heads_wide, out_wide, preferred_element_type=jnp.float32) + jnp.dot(heads_narrow, out_narrow, preferred_element_type=jnp.float32)
    stream = (projected + residual_in.astype(jnp.float32)).astype(jnp.bfloat16)
    stream_f = stream.astype(jnp.float32)
    normed = (stream_f * lax.rsqrt(lax.optimization_barrier(jnp.mean(stream_f * stream_f, axis=-1, keepdims=True)) + 1e-06) * ffn_gain).astype(jnp.bfloat16)
    flat_expert = expert_ids.reshape(-1)
    flat_token = jnp.repeat(jnp.arange(TOKENS, dtype=jnp.int32), 2)
    flat_weight = expert_weights.reshape(-1)
    slots = EXPERTS * CAP

    def one_expert(running, expert):
        chosen = flat_expert == expert
        count = jnp.sum(chosen.astype(jnp.int32))
        position = jnp.nonzero(chosen, size=slots, fill_value=0)[0].astype(jnp.int32)
        token_rows = flat_token[position]
        rows = normed[token_rows]
        gate_part = jnp.dot(rows, gate_weight[expert], preferred_element_type=jnp.float32)
        up_part = jnp.dot(rows, up_weight[expert], preferred_element_type=jnp.float32)
        hidden = (jax.nn.silu(gate_part) * up_part).astype(jnp.bfloat16)
        result = jnp.dot(hidden, down_weight[expert], preferred_element_type=jnp.float32)
        result = lax.optimization_barrier(result.astype(jnp.bfloat16)).astype(jnp.float32)
        share = jnp.where(jnp.arange(slots, dtype=jnp.int32) < count, flat_weight[position], 0.0)
        return (running.at[token_rows].add(share[:, None] * result), None)
    summed, _ = lax.scan(one_expert, jnp.zeros((TOKENS, D), jnp.float32), jnp.arange(EXPERTS, dtype=jnp.int32))
    return (stream_f + summed).astype(jnp.bfloat16)
```

```python
import functools
import math

import jax
import jax.numpy as jnp
from jax import lax
from jax.experimental import pallas as pl
from jax.experimental.pallas import tpu as pltpu
from jax.sharding import PartitionSpec as P

NEG_FILL = -1e30


def attend_kernel(flags, lam, *refs, count, diag, final, head_size, packed):
    q_ref = refs[0]
    blocks = [(refs[1 + 2 * b], refs[2 + 2 * b]) for b in range(count)]
    refs = refs[1 + 2 * count :]
    if not diag:
        acc_in, stat_in = refs[:2]
        refs = refs[2:]
    if final:
        out_ref, acc, peak, total = refs
    else:
        acc_out, stat_out, acc, peak, total = refs
    scale = head_size ** (-0.5) * math.log2(math.e)
    rows = q_ref.shape[0]
    head = pl.program_id(0)
    first_row = pl.program_id(1) * rows

    def lanes(column):
        return jnp.broadcast_to(column, (rows, 128))

    if not diag:
        acc[...] = acc_in[...]
        for m in range(2):
            peak[m] = lanes(stat_in[0, :, 2 * m : 2 * m + 1])
            total[m] = lanes(stat_in[0, :, 2 * m + 1 : 2 * m + 2])

    def update(k_ref, v_ref):
        values = v_ref[...]
        for m in range(2):
            if packed:
                side = lax.broadcasted_iota(jnp.int32, q_ref.shape, 1) // head_size
                query = jnp.where(side == m, q_ref[...], jnp.zeros_like(q_ref))
                keys = k_ref[...]
            else:
                query = q_ref[:, m * head_size : (m + 1) * head_size]
                keys = k_ref[:, m * head_size : (m + 1) * head_size]
            scores = (
                lax.dot_general(
                    query, keys, (((1,), (1,)), ((), ())), preferred_element_type=jnp.float32
                )
                * scale
            )
            if diag:
                row = first_row + lax.broadcasted_iota(jnp.int32, scores.shape, 0)
                col = lax.broadcasted_iota(jnp.int32, scores.shape, 1)
                scores = jnp.where(col <= row, scores, NEG_FILL)
            new_peak = jnp.max(scores, axis=1, keepdims=True)
            if not diag:
                old_peak = peak[m][:, :1]
                new_peak = jnp.maximum(old_peak, new_peak)
                factor = jnp.exp2(old_peak - new_peak)
            weights = jnp.exp2(scores - new_peak)
            new_total = jnp.sum(weights, axis=1, keepdims=True)
            read = jnp.dot(
                weights.astype(jnp.bfloat16), values, preferred_element_type=jnp.float32
            )
            if not diag:
                new_total = new_total + factor * total[m][:, :1]
                read = read + factor * acc[m]
            acc[m] = read
            peak[m] = lanes(new_peak)
            total[m] = lanes(new_total)

    for b in range(count):
        if diag:
            update(*blocks[b])
        else:
            pl.when(flags[b] == 1)(functools.partial(update, *blocks[b]))

    if final:
        mixed = acc[0] / total[0][:, :1] - lam[head] * (acc[1] / total[1][:, :1])
        out_ref[...] = (
            mixed * lax.rsqrt(jnp.mean(mixed * mixed, axis=1, keepdims=True) + 1e-06)
        ).astype(out_ref.dtype)
    else:
        acc_out[...] = acc[...]
        lane = lax.broadcasted_iota(jnp.int32, (rows, 128), 1)
        stat_out[0] = jnp.where(
            lane == 0,
            peak[0],
            jnp.where(lane == 1, total[0], jnp.where(lane == 2, peak[1], total[1])),
        )


def attend(query, pieces, flags, state, lam, head_size, value_size, key_col, value_col, final):
    diag = state is None
    tok_count, width = query.shape
    heads = width // (2 * head_size)
    block = math.gcd(tok_count, 256)
    packed = head_size % 128 != 0
    kb, vb = key_col // (2 * head_size), value_col // value_size
    q_spec = pl.BlockSpec((block, 2 * head_size), lambda h, i, *_: (i, h))
    acc_spec = pl.BlockSpec((2, block, value_size), lambda h, i, *_: (0, i, h))
    stat_spec = pl.BlockSpec((1, block, 128), lambda h, i, *_: (h, i, 0))
    in_specs, operands = [q_spec], [query]
    keys_seen = 0
    for piece, start, rows in pieces:
        keys_seen += rows
        at = start // rows
        in_specs += [
            pl.BlockSpec((rows, 2 * head_size), lambda h, i, *_, at=at: (at, kb + h)),
            pl.BlockSpec((rows, value_size), lambda h, i, *_, at=at: (at, vb + h)),
        ]
        operands += [piece, piece]
    aliases = {}
    if not diag:
        in_specs += [acc_spec, stat_spec]
        operands += list(state)
        if not final:
            aliases = {2 + len(operands) - 2: 0, 2 + len(operands) - 1: 1}
    if final:
        out_specs = pl.BlockSpec((block, value_size), lambda h, i, *_: (i, h))
        out_shape = jax.ShapeDtypeStruct((tok_count, heads * value_size), jnp.bfloat16)
    else:
        out_specs = (acc_spec, stat_spec)
        out_shape = (
            jax.ShapeDtypeStruct((2, tok_count, heads * value_size), jnp.float32),
            jax.ShapeDtypeStruct((heads, tok_count, 128), jnp.float32),
        )
    pairs = heads * tok_count * keys_seen * 2
    return pl.pallas_call(
        functools.partial(
            attend_kernel,
            count=len(pieces),
            diag=diag,
            final=final,
            head_size=head_size,
            packed=packed,
        ),
        grid_spec=pltpu.PrefetchScalarGridSpec(
            num_scalar_prefetch=2,
            grid=(heads, tok_count // block),
            in_specs=in_specs,
            out_specs=out_specs,
            scratch_shapes=[
                pltpu.VMEM((2, block, value_size), jnp.float32),
                pltpu.VMEM((2, block, 128), jnp.float32),
                pltpu.VMEM((2, block, 128), jnp.float32),
            ],
        ),
        out_shape=out_shape,
        input_output_aliases=aliases,
        compiler_params=pltpu.CompilerParams(vmem_limit_bytes=40 * 1024 * 1024),
        cost_estimate=pl.CostEstimate(
            flops=pairs * 1024,
            bytes_accessed=keys_seen * heads * (2 * head_size + value_size) * 2
            + tok_count * heads * value_size * 16,
            transcendentals=pairs,
        ),
    )(flags, lam, *operands)


MESH = pl.DeviceIdType.MESH


def pair_tables():
    orders = (
        ((0, 0), (1, 0), (2, 0), (3, 0), (1, 1), (2, 1), (3, 1), (2, 2), (3, 2), (3, 3)),
        ((1, 1), (2, 1), (1, 0), (2, 0), (3, 1), (3, 0), (0, 0), (2, 2), (3, 2), (3, 3)),
        ((2, 2), (3, 2), (2, 1), (3, 1), (2, 0), (3, 0), (3, 3), (1, 1), (1, 0), (0, 0)),
        ((3, 3), (3, 2), (3, 1), (3, 0), (2, 2), (2, 1), (2, 0), (1, 1), (1, 0), (0, 0)),
    )
    passing = ({2: 1, 6: 2, 8: 3}, {1: 0, 5: 2, 8: 3}, {1: 1, 3: 0, 5: 3}, {1: 2, 2: 1, 3: 0})
    words = []
    for level, order in enumerate(orders):
        row, seen_q, seen_k = [], {level}, set()
        for at, (i, j) in enumerate(order):
            word = i + 4 * j
            if i not in seen_q:
                word += 16
            if j not in seen_k:
                word += 32
            if all(pair[0] != i for pair in order[at + 1 :]):
                word += 64
            word += 128 * (passing[level][at] + 1 if at in passing[level] else 0)
            seen_q.add(i)
            seen_k.add(j)
            row.append(word)
        words.append(row)
    return words


def exchange_kernel(
    lam, qw_in, kw_in, vw_in, qn_in, kn_in, vn_in, wide_out, narrow_out,
    qw, kw, vw, qn, kn, vn, acc, peak, total, ow, on,
    own_sem, z_send, z_recv, x_send, x_recv, o_send, o_recv,
    *, levels, tp_count, heads,
):
    me_sp, me_tp = lax.axis_index("sp"), lax.axis_index("tp")
    level, side = me_sp // 2, me_sp % 2
    flavour = me_tp % 2
    tokens = qw_in.shape[0]
    share = tokens // tp_count
    kinds = (
        dict(ins=(qw_in, kw_in, vw_in), bufs=(qw, kw, vw), result=ow, out=wide_out),
        dict(ins=(qn_in, kn_in, vn_in), bufs=(qn, kn, vn), result=on, out=narrow_out),
    )
    for entry in kinds:
        entry["widths"] = tuple(ref.shape[1] // heads for ref in entry["ins"])

    def source(kind, what, head):
        width = kinds[kind]["widths"][what]
        return kinds[kind]["ins"][what].at[:, pl.ds(pl.multiple_of(head * width, width), width)]

    def slot(kind, what, at, other):
        block = at if what == 0 else 2 * at + other
        return kinds[kind]["bufs"][what].at[pl.ds(pl.multiple_of(block * tokens, tokens), tokens), :]

    def to_level(kind, what, target):
        return pltpu.make_async_remote_copy(
            src_ref=source(kind, what, target // 2),
            dst_ref=slot(kind, what, level, side),
            send_sem=z_send.at[what, target],
            recv_sem=z_recv.at[what, level],
            device_id=(2 * target + side, me_tp),
            device_id_type=MESH,
        )

    def from_level(kind, what, origin):
        ref = slot(kind, what, origin, side)
        return pltpu.make_async_remote_copy(
            src_ref=ref, dst_ref=ref, send_sem=z_send.at[what, origin],
            recv_sem=z_recv.at[what, origin], device_id=(2 * origin + side, me_tp), device_id_type=MESH,
        )

    def across(kind, what, at, own):
        return pltpu.make_async_remote_copy(
            src_ref=source(kind, what, level // 2) if own else slot(kind, what, at, side),
            dst_ref=slot(kind, what, at, side),
            send_sem=x_send.at[what, at],
            recv_sem=x_recv.at[what, at],
            device_id=(2 * level + 1 - side, me_tp),
            device_id_type=MESH,
        )

    def from_across(kind, what, at):
        ref = slot(kind, what, at, 1 - side)
        return pltpu.make_async_remote_copy(
            src_ref=ref, dst_ref=ref, send_sem=x_send.at[what, at], recv_sem=x_recv.at[what, at],
            device_id=(2 * level + 1 - side, me_tp), device_id_type=MESH,
        )

    def keep(kind, what):
        return pltpu.make_async_copy(
            source(kind, what, level // 2), slot(kind, what, level, side), own_sem.at[what]
        )

    def column(kind, at_level, at_tp):
        width = kinds[kind]["widths"][2]
        return pl.ds(pl.multiple_of((at_tp * heads + at_level // 2) * width, width), width)

    def result_rows(kind, i, part):
        return kinds[kind]["result"].at[
            pl.ds(pl.multiple_of(i * tokens + part * share, share), share), :
        ]

    def deliver(kind, i, part):
        return pltpu.make_async_remote_copy(
            src_ref=result_rows(kind, i, part),
            dst_ref=kinds[kind]["out"].at[:, column(kind, level, me_tp)],
            send_sem=o_send.at[i, part],
            recv_sem=o_recv.at[level, me_tp],
            device_id=(2 * i + side, part),
            device_id_type=MESH,
        )

    def keep_result(kind, part):
        return pltpu.make_async_copy(
            result_rows(kind, level, part),
            kinds[kind]["out"].at[:, column(kind, level, me_tp)],
            own_sem.at[3],
        )

    def of_kind(at_level, body):
        kind_here = (at_level + flavour) % 2
        for kind in range(2):
            pl.when(kind_here == kind)(functools.partial(body, kind))

    def begin_own(kind):
        for what in (1, 2):
            across(kind, what, level, True).start()
        for what in range(3):
            keep(kind, what).start()

    of_kind(level, begin_own)

    def over_targets(whats, body):
        for step in range(1, levels):
            for target in (level + step, level - step):
                rising = target > level

                def one(target=target):
                    def at_kind(kind):
                        for what in whats:
                            body(to_level(kind, what, target))

                    of_kind(target, at_kind)

                yield rising, jnp.logical_and(target >= 0, target < levels), one

    early_up = list(over_targets((1, 2), lambda copy: copy.start()))
    early_down = list(over_targets((0,), lambda copy: copy.start()))
    for rising, valid, one in early_up:
        pl.when(jnp.logical_and(valid, rising))(one)
    for rising, valid, one in early_down:
        pl.when(jnp.logical_and(valid, jnp.logical_not(rising)))(one)
    for rising, valid, one in early_up:
        pl.when(jnp.logical_and(valid, jnp.logical_not(rising)))(one)
    for rising, valid, one in early_down:
        pl.when(jnp.logical_and(valid, rising))(one)

    words = pair_tables()
    steps = len(words[0])
    here = [
        sum(jnp.where(level == at, words[at][step], 0) for at in range(levels)) for step in range(steps)
    ]

    def run(kind):
        q_buf, k_buf, v_buf = kinds[kind]["bufs"]
        head_size = q_buf.shape[1] // 2
        value_size = v_buf.shape[1]
        packed = head_size % 128 != 0
        scale = head_size ** (-0.5) * math.log2(math.e)
        rows = math.gcd(tokens, 384)

        def clear(at, carry):
            span = pl.ds(pl.multiple_of(at * rows, rows), rows)
            for m in range(2):
                acc[m, span, :value_size] = jnp.zeros((rows, value_size), jnp.float32)
                peak[m, span, :] = jnp.full((rows, 128), NEG_FILL, jnp.float32)
                total[m, span, :] = jnp.zeros((rows, 128), jnp.float32)
            return carry

        lax.fori_loop(0, levels * tokens // rows, clear, 0)
        for what in range(3):
            keep(kind, what).wait()

        def update(q_at, k_at, count, edge):
            q_span = pl.ds(pl.multiple_of(q_at, rows), rows)
            k_span = pl.ds(pl.multiple_of(k_at, tokens), count)
            values = v_buf[k_span, :]
            found = []
            for m in range(2):
                if packed:
                    query, keys = q_buf[q_span, :], k_buf[k_span, :]
                    half = lax.broadcasted_iota(jnp.int32, query.shape, 1) // head_size
                    query = jnp.where(half == m, query, jnp.zeros_like(query))
                else:
                    query = q_buf[q_span, m * head_size : (m + 1) * head_size]
                    keys = k_buf[k_span, m * head_size : (m + 1) * head_size]
                found.append(
                    lax.dot_general(
                        query, keys, (((1,), (1,)), ((), ())), preferred_element_type=jnp.float32
                    )
                )
            for m in range(2):
                scores = found[m]
                if edge is not None:
                    row = lax.broadcasted_iota(jnp.int32, scores.shape, 0)
                    col = lax.broadcasted_iota(jnp.int32, scores.shape, 1)
                    scores = jnp.where(col - row <= edge, scores, NEG_FILL)
                old_peak = peak[m, q_span, :]
                new_peak = jnp.maximum(old_peak, jnp.max(scores, axis=1, keepdims=True) * scale)
                weights = jnp.exp2(scores * scale - jnp.concatenate([new_peak] * (count // 128), axis=1))
                factor = jnp.exp2(old_peak - new_peak)
                partial = weights[:, :128]
                for piece in range(1, count // 128):
                    partial = partial + weights[:, piece * 128 : (piece + 1) * 128]
                read = jnp.dot(weights.astype(jnp.bfloat16), values, preferred_element_type=jnp.float32)
                spread = factor if value_size == 128 else jnp.concatenate([factor] * (value_size // 128), axis=1)
                acc[m, q_span, :value_size] = acc[m, q_span, :value_size] * spread + read
                total[m, q_span, :] = total[m, q_span, :] * factor + partial
                peak[m, q_span, :] = new_peak

        def one_step(step, carry):
            word = sum(jnp.where(step == at, here[at], 0) for at in range(steps))
            i, j = word % 4, word // 4 % 4
            passed = word // 128

            @pl.when(passed > 0)
            def _():
                for what in (1, 2):
                    from_level(kind, what, passed - 1).wait_recv()
                    across(kind, what, passed - 1, False).start()

            @pl.when(word // 16 % 2 == 1)
            def _():
                from_level(kind, 0, i).wait_recv()

            @pl.when(word // 32 % 2 == 1)
            def _():
                for what in (1, 2):
                    from_across(kind, what, j).wait_recv()

            @pl.when(i != j)
            def _():
                def tile(at, inner):
                    update(i * tokens + at * rows, 2 * j * tokens, 2 * tokens, None)
                    return inner

                lax.fori_loop(0, tokens // rows, tile, 0)

            @pl.when(i == j)
            def _():
                def tile(at, inner):
                    block, q_tile = at // (tokens // rows), at % (tokens // rows)
                    update(
                        i * tokens + q_tile * rows,
                        (2 * i + block) * tokens,
                        tokens,
                        q_tile * rows + (side - block) * tokens,
                    )
                    return inner

                lax.fori_loop(0, (side + 1) * (tokens // rows), tile, 0)

            @pl.when(word // 64 % 2 == 1)
            def _():
                result = kinds[kind]["result"]
                weight = lam[kind, level // 2]

                def finish(at, inner):
                    span = pl.ds(pl.multiple_of(i * tokens + at * rows, rows), rows)
                    first, second = (
                        acc[m, span, :value_size] / jnp.sum(total[m, span, :], axis=1, keepdims=True)
                        for m in range(2)
                    )
                    mixed = first - weight * second
                    result[span, :] = (
                        mixed * lax.rsqrt(jnp.mean(mixed * mixed, axis=1, keepdims=True) + 1e-06)
                    ).astype(result.dtype)
                    return inner

                lax.fori_loop(0, tokens // rows, finish, 0)
                for part in range(tp_count):
                    mine = jnp.logical_and(i == level, me_tp == part)
                    pl.when(mine)(lambda part=part: keep_result(kind, part).start())
                    pl.when(jnp.logical_not(mine))(lambda part=part: deliver(kind, i, part).start())

            return carry

        lax.fori_loop(0, steps, one_step, 0)

        for what in (1, 2):
            for at in range(levels):
                pl.when(level == at)(lambda what=what, at=at: across(kind, what, at, True).wait_send())
                pl.when(level != at)(lambda what=what, at=at: across(kind, what, at, False).wait_send())
        for i in range(levels):
            for part in range(tp_count):
                mine = jnp.logical_and(i == level, me_tp == part)
                pl.when(mine)(lambda part=part: keep_result(kind, part).wait())
                pl.when(jnp.logical_not(mine))(lambda i=i, part=part: deliver(kind, i, part).wait_send())

    of_kind(level, run)

    for rising, valid, one in over_targets((0, 1, 2), lambda copy: copy.wait_send()):
        pl.when(valid)(one)
    for origin in range(levels):
        for part in range(tp_count):
            kind = (origin + part) % 2
            ref = kinds[kind]["out"].at[:, column(kind, origin, part)]

            @pl.when(jnp.logical_not(jnp.logical_and(origin == level, part == me_tp)))
            def _(origin=origin, part=part, ref=ref):
                pltpu.make_async_remote_copy(
                    src_ref=ref, dst_ref=ref, send_sem=o_send.at[origin, part],
                    recv_sem=o_recv.at[origin, part], device_id=(2 * origin + side, part),
                    device_id_type=MESH,
                ).wait_recv()


def exchange_attention(lam, qw, kw, vw, qn, kn, vn, levels, tp_count, heads):
    tokens = qw.shape[0]
    share = tokens // tp_count
    wide, narrow = [x.shape[1] // heads for x in (qw, kw, vw)], [x.shape[1] // heads for x in (qn, kn, vn)]
    most = max(wide[2], narrow[2])
    rows = levels * tokens

    def buffers(widths):
        return [
            pltpu.VMEM((rows, widths[0]), jnp.bfloat16),
            pltpu.VMEM((2 * rows, widths[1]), jnp.bfloat16),
            pltpu.VMEM((2 * rows, widths[2]), jnp.bfloat16),
        ]

    pairs = 2 * rows * rows * 2
    return pl.pallas_call(
        functools.partial(exchange_kernel, levels=levels, tp_count=tp_count, heads=heads),
        in_specs=[pl.BlockSpec(memory_space=pltpu.SMEM)] + [pl.BlockSpec(memory_space=pl.ANY)] * 6,
        out_specs=[pl.BlockSpec(memory_space=pltpu.VMEM)] * 2,
        out_shape=[
            jax.ShapeDtypeStruct((share, tp_count * heads * wide[2]), jnp.bfloat16),
            jax.ShapeDtypeStruct((share, tp_count * heads * narrow[2]), jnp.bfloat16),
        ],
        scratch_shapes=buffers(wide)
        + buffers(narrow)
        + [
            pltpu.VMEM((2, rows, most), jnp.float32),
            pltpu.VMEM((2, rows, 128), jnp.float32),
            pltpu.VMEM((2, rows, 128), jnp.float32),
            pltpu.VMEM((rows, wide[2]), jnp.bfloat16),
            pltpu.VMEM((rows, narrow[2]), jnp.bfloat16),
            pltpu.SemaphoreType.DMA((4,)),
            pltpu.SemaphoreType.DMA((3, levels)),
            pltpu.SemaphoreType.DMA((3, levels)),
            pltpu.SemaphoreType.DMA((3, levels)),
            pltpu.SemaphoreType.DMA((3, levels)),
            pltpu.SemaphoreType.DMA((levels, tp_count)),
            pltpu.SemaphoreType.DMA((levels, tp_count)),
        ],
        compiler_params=pltpu.CompilerParams(
            vmem_limit_bytes=58 * 1024 * 1024, has_side_effects=True
        ),
        cost_estimate=pl.CostEstimate(
            flops=pairs * 1024, bytes_accessed=tokens * 4096 * 8, transcendentals=pairs
        ),
    )(lam, qw, kw, vw, qn, kn, vn)


def ring_order(count):
    return list(range(0, count, 2)) + list(range(1, count, 2))[::-1]


def ring_attention(
    query_wide, key_wide, value_wide, query_narrow, key_narrow, value_narrow, mix_lambda
):
    tok_count, local_heads, _ = query_wide.shape
    size_wide = query_wide.shape[2] // 2
    size_narrow = query_narrow.shape[2] // 2

    value_wide_size, value_narrow_size = value_wide.shape[2], value_narrow.shape[2]
    flat = lambda member: member.reshape(tok_count, -1)
    own = jnp.concatenate(
        [flat(key_wide), flat(value_wide), flat(key_narrow), flat(value_narrow)], axis=1
    )
    wide_q, narrow_q = flat(query_wide), flat(query_narrow)
    wide_v_col = local_heads * 2 * size_wide
    narrow_k_col = wide_v_col + local_heads * value_wide_size
    narrow_v_col = narrow_k_col + local_heads * 2 * size_narrow

    count = lax.axis_size("sp")
    order = ring_order(count)
    place = [order.index(device) for device in range(count)]
    me = lax.axis_index("sp")
    order_table = jnp.array(order, jnp.int32)
    my_place = jnp.array(place, jnp.int32)[me]
    forward = [(order[i], order[(i + 1) % count]) for i in range(count)]
    backward = [(b, a) for a, b in forward]

    def source_flag(shift):
        return (order_table[(my_place + shift) % count] < me).astype(jnp.int32)

    def both(pieces, flags, states, final=False):
        return (
            attend(
                wide_q, pieces, flags, states[0], mix_lambda[0], size_wide, value_wide_size,
                0, wide_v_col, final,
            ),
            attend(
                narrow_q, pieces, flags, states[1], mix_lambda[1], size_narrow, value_narrow_size,
                narrow_k_col, narrow_v_col, final,
            ),
        )

    half = tok_count // 2
    pieces = [(own, 0, tok_count)]
    flags = jnp.ones((2,), jnp.int32)
    states = (None, None)
    left = right = own
    for step in range(1, count // 2 + 1):
        if step < count // 2:
            left = lax.ppermute(left, "sp", forward)
            right = lax.ppermute(right, "sp", backward)
            coming = [(left, 0, tok_count), (right, 0, tok_count)]
        else:
            coming = [
                (lax.ppermute(left[:half], "sp", forward), 0, half),
                (lax.ppermute(right[half:], "sp", backward), 0, half),
            ]
        states = both(pieces, flags, states)
        arrived_now, states = lax.optimization_barrier(
            (tuple(piece for piece, _, _ in coming), states)
        )
        pieces = [(arrived_now[i], 0, coming[i][2]) for i in range(2)]
        left, right = arrived_now
        flags = jnp.stack([source_flag(-step), source_flag(step)])
    heads_wide, heads_narrow = both(pieces, flags, states, final=True)
    return (
        lax.all_to_all(heads_wide, "tp", split_axis=0, concat_axis=1, tiled=True),
        lax.all_to_all(heads_narrow, "tp", split_axis=0, concat_axis=1, tiled=True),
    )


def shards(
    query_wide,
    key_wide,
    value_wide,
    query_narrow,
    key_narrow,
    value_narrow,
    mix_lambda,
    residual_in,
    out_wide,
    out_narrow,
    ffn_gain,
    expert_ids,
    expert_weights,
    gate_weight,
    up_weight,
    down_weight,
):
    tok_count, local_heads, _ = query_wide.shape
    tp_size, sp_size = lax.axis_size("tp"), lax.axis_size("sp")
    attention_args = (
        query_wide, key_wide, value_wide, query_narrow, key_narrow, value_narrow, mix_lambda
    )
    if sp_size == 8 and local_heads * 4 == sp_size and tp_size % 2 == 0:
        flat = [member.reshape(tok_count, -1) for member in attention_args[:6]]
        mine_wide, mine_narrow = exchange_attention(
            mix_lambda, *flat, sp_size // 2, tp_size, local_heads
        )
    else:
        mine_wide, mine_narrow = ring_attention(*attention_args)
    local_rows = tok_count // tp_size
    whole_wide, whole_narrow = (
        lax.all_gather(out_wide, "tp", axis=0, tiled=True),
        lax.all_gather(out_narrow, "tp", axis=0, tiled=True),
    )
    projected = jnp.dot(mine_wide, whole_wide, preferred_element_type=jnp.float32) + jnp.dot(
        mine_narrow, whole_narrow, preferred_element_type=jnp.float32
    )
    stream = (projected + residual_in.astype(jnp.float32)).astype(jnp.bfloat16)
    stream_f = stream.astype(jnp.float32)
    normed = (
        stream_f
        * lax.rsqrt(jnp.mean(stream_f * stream_f, axis=-1, keepdims=True) + 1e-06)
        * ffn_gain
    ).astype(jnp.bfloat16)
    experts_all = lax.axis_size("sp") * tp_size
    capacity = max(2, 4 * local_rows // experts_all)
    model_width = normed.shape[1]
    flat_expert = expert_ids.reshape(-1)
    expert_hot = (flat_expert[:, None] == jnp.arange(experts_all, dtype=jnp.int32)[None, :]).astype(
        jnp.int32
    )
    slot_rank = jnp.sum((jnp.cumsum(expert_hot, axis=0) - 1) * expert_hot, axis=1)
    flat_slot = flat_expert * capacity + slot_rank
    slot_ids = jnp.arange(experts_all * capacity, dtype=jnp.int32)
    placed = slot_ids[:, None] == flat_slot[None, :]
    dispatch = jnp.any(placed.reshape(experts_all * capacity, local_rows, 2), axis=2).astype(
        jnp.bfloat16
    )
    outgoing = jnp.dot(dispatch, normed, preferred_element_type=jnp.float32).astype(jnp.bfloat16)
    outgoing = outgoing.reshape(experts_all, capacity, model_width)
    arrived = lax.all_to_all(outgoing, ("sp", "tp"), split_axis=0, concat_axis=0, tiled=True)
    sources, items, width = arrived.shape
    flat_rows = arrived.reshape(sources * items, width)
    gate_part = jnp.dot(flat_rows, gate_weight[0], preferred_element_type=jnp.float32)
    up_part = jnp.dot(flat_rows, up_weight[0], preferred_element_type=jnp.float32)
    hidden = (jax.nn.silu(gate_part) * up_part).astype(jnp.bfloat16)
    result = jnp.dot(hidden, down_weight[0], preferred_element_type=jnp.float32).astype(
        jnp.bfloat16
    )
    returned = lax.all_to_all(
        result.reshape(sources, items, width), ("sp", "tp"), split_axis=0, concat_axis=0, tiled=True
    )
    slot_hot = (flat_slot[:, None] == slot_ids[None, :]).astype(
        jnp.float32
    ) * expert_weights.reshape(-1)[:, None]
    combine = jnp.sum(slot_hot.reshape(local_rows, 2, experts_all * capacity), axis=1)
    summed = jnp.dot(
        combine,
        returned.reshape(experts_all * capacity, model_width).astype(jnp.float32),
        precision=lax.Precision.HIGHEST,
    )
    return (stream_f + summed).astype(jnp.bfloat16)


def solution(mesh):
    return jax.shard_map(
        shards,
        mesh=mesh,
        in_specs=(
            P("sp", "tp", None),
            P("sp", "tp", None),
            P("sp", "tp", None),
            P("sp", "tp", None),
            P("sp", "tp", None),
            P("sp", "tp", None),
            P(None, "tp"),
            P(("sp", "tp"), None),
            P("tp", None),
            P("tp", None),
            P(),
            P(("sp", "tp"), None),
            P(("sp", "tp"), None),
            P(("sp", "tp"), None, None),
            P(("sp", "tp"), None, None),
            P(("sp", "tp"), None, None),
        ),
        out_specs=P(("sp", "tp"), None),
        check_vma=False,
    )
```

```python
import functools
import math

import jax
import jax.numpy as jnp
from jax import lax
from jax.experimental import pallas as pl
from jax.experimental.pallas import tpu as pltpu
from jax.sharding import PartitionSpec as P

NEG_FILL = -1e30
GROUP = 4


def attend_kernel(flags, lam, *refs, count, diag, final, head_size, packed):
    q_ref = refs[0]
    blocks = [(refs[1 + 2 * b], refs[2 + 2 * b]) for b in range(count)]
    refs = refs[1 + 2 * count :]
    if not diag:
        acc_in, stat_in = refs[:2]
        refs = refs[2:]
    if final:
        out_ref, acc, peak, total = refs
    else:
        acc_out, stat_out, acc, peak, total = refs
    scale = head_size ** (-0.5) * math.log2(math.e)
    rows = q_ref.shape[0]
    head = pl.program_id(0)
    first_row = pl.program_id(1) * rows

    def lanes(column):
        return jnp.broadcast_to(column, (rows, 128))

    if not diag:
        acc[...] = acc_in[...]
        for m in range(2):
            peak[m] = lanes(stat_in[0, :, 2 * m : 2 * m + 1])
            total[m] = lanes(stat_in[0, :, 2 * m + 1 : 2 * m + 2])

    def update(k_ref, v_ref):
        values = v_ref[...]
        for m in range(2):
            if packed:
                side = lax.broadcasted_iota(jnp.int32, q_ref.shape, 1) // head_size
                query = jnp.where(side == m, q_ref[...], jnp.zeros_like(q_ref))
                keys = k_ref[...]
            else:
                query = q_ref[:, m * head_size : (m + 1) * head_size]
                keys = k_ref[:, m * head_size : (m + 1) * head_size]
            scores = (
                lax.dot_general(
                    query, keys, (((1,), (1,)), ((), ())), preferred_element_type=jnp.float32
                )
                * scale
            )
            if diag:
                row = first_row + lax.broadcasted_iota(jnp.int32, scores.shape, 0)
                col = lax.broadcasted_iota(jnp.int32, scores.shape, 1)
                scores = jnp.where(col <= row, scores, NEG_FILL)
            new_peak = jnp.max(scores, axis=1, keepdims=True)
            if not diag:
                old_peak = peak[m][:, :1]
                new_peak = jnp.maximum(old_peak, new_peak)
                factor = jnp.exp2(old_peak - new_peak)
            weights = jnp.exp2(scores - new_peak)
            new_total = jnp.sum(weights, axis=1, keepdims=True)
            read = jnp.dot(
                weights.astype(jnp.bfloat16), values, preferred_element_type=jnp.float32
            )
            if not diag:
                new_total = new_total + factor * total[m][:, :1]
                read = read + factor * acc[m]
            acc[m] = read
            peak[m] = lanes(new_peak)
            total[m] = lanes(new_total)

    for b in range(count):
        if diag:
            update(*blocks[b])
        else:
            pl.when(flags[b] == 1)(functools.partial(update, *blocks[b]))

    if final:
        mixed = acc[0] / total[0][:, :1] - lam[head] * (acc[1] / total[1][:, :1])
        out_ref[...] = (
            mixed * lax.rsqrt(jnp.mean(mixed * mixed, axis=1, keepdims=True) + 1e-06)
        ).astype(out_ref.dtype)
    else:
        acc_out[...] = acc[...]
        lane = lax.broadcasted_iota(jnp.int32, (rows, 128), 1)
        stat_out[0] = jnp.where(
            lane == 0,
            peak[0],
            jnp.where(lane == 1, total[0], jnp.where(lane == 2, peak[1], total[1])),
        )


def attend(query, pieces, flags, state, lam, head_size, value_size, key_col, value_col, final):
    diag = state is None
    tok_count, width = query.shape
    heads = width // (2 * head_size)
    block = math.gcd(tok_count, 256)
    packed = head_size % 128 != 0
    kb, vb = key_col // (2 * head_size), value_col // value_size
    q_spec = pl.BlockSpec((block, 2 * head_size), lambda h, i, *_: (i, h))
    acc_spec = pl.BlockSpec((2, block, value_size), lambda h, i, *_: (0, i, h))
    stat_spec = pl.BlockSpec((1, block, 128), lambda h, i, *_: (h, i, 0))
    in_specs, operands = [q_spec], [query]
    keys_seen = 0
    for piece, start, rows in pieces:
        keys_seen += rows
        at = start // rows
        in_specs += [
            pl.BlockSpec((rows, 2 * head_size), lambda h, i, *_, at=at: (at, kb + h)),
            pl.BlockSpec((rows, value_size), lambda h, i, *_, at=at: (at, vb + h)),
        ]
        operands += [piece, piece]
    aliases = {}
    if not diag:
        in_specs += [acc_spec, stat_spec]
        operands += list(state)
        if not final:
            aliases = {2 + len(operands) - 2: 0, 2 + len(operands) - 1: 1}
    if final:
        out_specs = pl.BlockSpec((block, value_size), lambda h, i, *_: (i, h))
        out_shape = jax.ShapeDtypeStruct((tok_count, heads * value_size), jnp.bfloat16)
    else:
        out_specs = (acc_spec, stat_spec)
        out_shape = (
            jax.ShapeDtypeStruct((2, tok_count, heads * value_size), jnp.float32),
            jax.ShapeDtypeStruct((heads, tok_count, 128), jnp.float32),
        )
    pairs = heads * tok_count * keys_seen * 2
    return pl.pallas_call(
        functools.partial(
            attend_kernel,
            count=len(pieces),
            diag=diag,
            final=final,
            head_size=head_size,
            packed=packed,
        ),
        grid_spec=pltpu.PrefetchScalarGridSpec(
            num_scalar_prefetch=2,
            grid=(heads, tok_count // block),
            in_specs=in_specs,
            out_specs=out_specs,
            scratch_shapes=[
                pltpu.VMEM((2, block, value_size), jnp.float32),
                pltpu.VMEM((2, block, 128), jnp.float32),
                pltpu.VMEM((2, block, 128), jnp.float32),
            ],
        ),
        out_shape=out_shape,
        input_output_aliases=aliases,
        compiler_params=pltpu.CompilerParams(vmem_limit_bytes=40 * 1024 * 1024),
        cost_estimate=pl.CostEstimate(
            flops=pairs * 1024,
            bytes_accessed=keys_seen * heads * (2 * head_size + value_size) * 2
            + tok_count * heads * value_size * 16,
            transcendentals=pairs,
        ),
    )(flags, lam, *operands)


MESH = pl.DeviceIdType.MESH


def pair_tables():
    orders = (
        ((0, 0), (1, 0), (2, 0), (3, 0), (1, 1), (2, 1), (3, 1), (2, 2), (3, 2), (3, 3)),
        ((1, 1), (2, 1), (1, 0), (2, 0), (3, 1), (3, 0), (0, 0), (2, 2), (3, 2), (3, 3)),
        ((2, 2), (3, 2), (2, 1), (3, 1), (2, 0), (3, 0), (3, 3), (1, 1), (1, 0), (0, 0)),
        ((3, 3), (3, 2), (3, 1), (3, 0), (2, 2), (2, 1), (2, 0), (1, 1), (1, 0), (0, 0)),
    )
    passing = ({2: 1, 6: 2, 8: 3}, {1: 0, 5: 2, 8: 3}, {1: 1, 3: 0, 5: 3}, {1: 2, 2: 1, 3: 0})
    words = []
    for level, order in enumerate(orders):
        row, seen_q, seen_k = [], {level}, set()
        for at, (i, j) in enumerate(order):
            word = i + 4 * j
            if i not in seen_q:
                word += 16
            if j not in seen_k:
                word += 32
            if all(pair[0] != i for pair in order[at + 1 :]):
                word += 64
            word += 128 * (passing[level][at] + 1 if at in passing[level] else 0)
            seen_q.add(i)
            seen_k.add(j)
            row.append(word)
        words.append(row)
    return words


def exchange_kernel(
    lam, qw_in, kw_in, vw_in, qn_in, kn_in, vn_in, pw_in, pn_in, residual, gain, stream, normed,
    qw, kw, vw, qn, kn, vn, acc, peak, total, ow, on, wide_out, narrow_out, pw, pn,
    own_sem, z_send, z_recv, x_send, x_recv, o_send, o_recv, p_send, p_recv,
    *, levels, tp_count, heads,
):
    me_sp, me_tp = lax.axis_index("sp"), lax.axis_index("tp")
    level, side = me_sp // 2, me_sp % 2
    flavour = me_tp % 2
    tokens = qw_in.shape[0]
    share = tokens // tp_count
    kinds = (
        dict(ins=(qw_in, kw_in, vw_in), bufs=(qw, kw, vw), result=ow, out=wide_out),
        dict(ins=(qn_in, kn_in, vn_in), bufs=(qn, kn, vn), result=on, out=narrow_out),
    )
    for entry in kinds:
        entry["widths"] = tuple(ref.shape[1] // heads for ref in entry["ins"])

    def source(kind, what, head):
        width = kinds[kind]["widths"][what]
        return kinds[kind]["ins"][what].at[:, pl.ds(pl.multiple_of(head * width, width), width)]

    def slot(kind, what, at, other):
        block = at if what == 0 else 2 * at + other
        return kinds[kind]["bufs"][what].at[pl.ds(pl.multiple_of(block * tokens, tokens), tokens), :]

    def to_level(kind, what, target):
        return pltpu.make_async_remote_copy(
            src_ref=source(kind, what, target // 2),
            dst_ref=slot(kind, what, level, side),
            send_sem=z_send.at[what, target],
            recv_sem=z_recv.at[what, level],
            device_id=(2 * target + side, me_tp),
            device_id_type=MESH,
        )

    def from_level(kind, what, origin):
        ref = slot(kind, what, origin, side)
        return pltpu.make_async_remote_copy(
            src_ref=ref, dst_ref=ref, send_sem=z_send.at[what, origin],
            recv_sem=z_recv.at[what, origin], device_id=(2 * origin + side, me_tp), device_id_type=MESH,
        )

    def across(kind, what, at, own):
        return pltpu.make_async_remote_copy(
            src_ref=source(kind, what, level // 2) if own else slot(kind, what, at, side),
            dst_ref=slot(kind, what, at, side),
            send_sem=x_send.at[what, at],
            recv_sem=x_recv.at[what, at],
            device_id=(2 * level + 1 - side, me_tp),
            device_id_type=MESH,
        )

    def from_across(kind, what, at):
        ref = slot(kind, what, at, 1 - side)
        return pltpu.make_async_remote_copy(
            src_ref=ref, dst_ref=ref, send_sem=x_send.at[what, at], recv_sem=x_recv.at[what, at],
            device_id=(2 * level + 1 - side, me_tp), device_id_type=MESH,
        )

    def keep(kind, what):
        return pltpu.make_async_copy(
            source(kind, what, level // 2), slot(kind, what, level, side), own_sem.at[what]
        )

    def column(kind, at_level, at_tp):
        width = kinds[kind]["widths"][2]
        return pl.ds(pl.multiple_of((at_tp * heads + at_level // 2) * width, width), width)

    def result_rows(kind, i, part):
        return kinds[kind]["result"].at[
            pl.ds(pl.multiple_of(i * tokens + part * share, share), share), :
        ]

    def deliver(kind, i, part):
        return pltpu.make_async_remote_copy(
            src_ref=result_rows(kind, i, part),
            dst_ref=kinds[kind]["out"].at[:, column(kind, level, me_tp)],
            send_sem=o_send.at[i, part],
            recv_sem=o_recv.at[level, me_tp],
            device_id=(2 * i + side, part),
            device_id_type=MESH,
        )

    def keep_result(kind, part):
        return pltpu.make_async_copy(
            result_rows(kind, level, part),
            kinds[kind]["out"].at[:, column(kind, level, me_tp)],
            own_sem.at[3],
        )

    def of_kind(at_level, body):
        kind_here = (at_level + flavour) % 2
        for kind in range(2):
            pl.when(kind_here == kind)(functools.partial(body, kind))

    def begin_own(kind):
        for what in (1, 2):
            across(kind, what, level, True).start()
        for what in range(3):
            keep(kind, what).start()

    of_kind(level, begin_own)

    tp_y, tp_core = me_tp // 2, me_tp % 2
    sibling, peer = 2 * tp_y + 1 - tp_core, 2 * (1 - tp_y) + tp_core
    projections = ((pw_in, pw), (pn_in, pn))

    def shard_of(which, at_tp):
        rows = projections[which][0].shape[0]
        return projections[which][1].at[pl.ds(pl.multiple_of(at_tp * rows, rows), rows), :]

    def share_shard(which, at, target, owner, own):
        return pltpu.make_async_remote_copy(
            src_ref=projections[which][0] if own else shard_of(which, owner),
            dst_ref=shard_of(which, owner),
            send_sem=p_send.at[which, at],
            recv_sem=p_recv.at[which, at],
            device_id=(me_sp, target),
            device_id_type=MESH,
        )

    def keep_shard(which):
        return pltpu.make_async_copy(
            projections[which][0], shard_of(which, me_tp), own_sem.at[4 + which]
        )

    def shard_copy(which, at):
        if at == 2:
            return share_shard(which, 2, sibling, peer, False)
        return share_shard(which, at, (sibling, peer)[at], me_tp, True)

    for which in range(2):
        keep_shard(which).start()
        for at in range(2):
            shard_copy(which, at).start()

    def over_targets(whats, body):
        for step in range(1, levels):
            for target in (level + step, level - step):
                rising = target > level

                def one(target=target):
                    def at_kind(kind):
                        for what in whats:
                            body(to_level(kind, what, target))

                    of_kind(target, at_kind)

                yield rising, jnp.logical_and(target >= 0, target < levels), one

    early_up = list(over_targets((1, 2), lambda copy: copy.start()))
    early_down = list(over_targets((0,), lambda copy: copy.start()))
    for rising, valid, one in early_up:
        pl.when(jnp.logical_and(valid, rising))(one)
    for rising, valid, one in early_down:
        pl.when(jnp.logical_and(valid, jnp.logical_not(rising)))(one)
    for rising, valid, one in early_up:
        pl.when(jnp.logical_and(valid, jnp.logical_not(rising)))(one)
    for rising, valid, one in early_down:
        pl.when(jnp.logical_and(valid, rising))(one)

    words = pair_tables()
    steps = len(words[0])
    here = [
        sum(jnp.where(level == at, words[at][step], 0) for at in range(levels)) for step in range(steps)
    ]

    def run(kind):
        q_buf, k_buf, v_buf = kinds[kind]["bufs"]
        head_size = q_buf.shape[1] // 2
        value_size = v_buf.shape[1]
        packed = head_size % 128 != 0
        scale = head_size ** (-0.5) * math.log2(math.e)
        rows = math.gcd(tokens, 384)

        def clear(at, carry):
            span = pl.ds(pl.multiple_of(at * rows, rows), rows)
            for m in range(2):
                acc[m, span, :value_size] = jnp.zeros((rows, value_size), jnp.float32)
                peak[m, span, :] = jnp.full((rows, 128), NEG_FILL, jnp.float32)
                total[m, span, :] = jnp.zeros((rows, 128), jnp.float32)
            return carry

        lax.fori_loop(0, levels * tokens // rows, clear, 0)
        for what in range(3):
            keep(kind, what).wait()

        def update(q_at, k_at, count, edge):
            q_span = pl.ds(pl.multiple_of(q_at, rows), rows)
            k_span = pl.ds(pl.multiple_of(k_at, tokens), count)
            values = v_buf[k_span, :]
            found = []
            for m in range(2):
                if packed:
                    query, keys = q_buf[q_span, :], k_buf[k_span, :]
                    half = lax.broadcasted_iota(jnp.int32, query.shape, 1) // head_size
                    query = jnp.where(half == m, query, jnp.zeros_like(query))
                else:
                    query = q_buf[q_span, m * head_size : (m + 1) * head_size]
                    keys = k_buf[k_span, m * head_size : (m + 1) * head_size]
                found.append(
                    lax.dot_general(
                        query, keys, (((1,), (1,)), ((), ())), preferred_element_type=jnp.float32
                    )
                )
            for m in range(2):
                scores = found[m]
                if edge is not None:
                    row = lax.broadcasted_iota(jnp.int32, scores.shape, 0)
                    col = lax.broadcasted_iota(jnp.int32, scores.shape, 1)
                    scores = jnp.where(col - row <= edge, scores, NEG_FILL)
                old_peak = peak[m, q_span, :]
                new_peak = jnp.maximum(old_peak, jnp.max(scores, axis=1, keepdims=True) * scale)
                weights = jnp.exp2(scores * scale - jnp.concatenate([new_peak] * (count // 128), axis=1))
                factor = jnp.exp2(old_peak - new_peak)
                partial = weights[:, :128]
                for piece in range(1, count // 128):
                    partial = partial + weights[:, piece * 128 : (piece + 1) * 128]
                read = jnp.dot(weights.astype(jnp.bfloat16), values, preferred_element_type=jnp.float32)
                spread = factor if value_size == 128 else jnp.concatenate([factor] * (value_size // 128), axis=1)
                acc[m, q_span, :value_size] = acc[m, q_span, :value_size] * spread + read
                total[m, q_span, :] = total[m, q_span, :] * factor + partial
                peak[m, q_span, :] = new_peak

        def one_step(step, carry):
            word = sum(jnp.where(step == at, here[at], 0) for at in range(steps))
            i, j = word % 4, word // 4 % 4
            passed = word // 128

            @pl.when(passed > 0)
            def _():
                for what in (1, 2):
                    from_level(kind, what, passed - 1).wait_recv()
                    across(kind, what, passed - 1, False).start()

            @pl.when(word // 16 % 2 == 1)
            def _():
                from_level(kind, 0, i).wait_recv()

            @pl.when(word // 32 % 2 == 1)
            def _():
                for what in (1, 2):
                    from_across(kind, what, j).wait_recv()

            @pl.when(i != j)
            def _():
                def tile(at, inner):
                    update(i * tokens + at * rows, 2 * j * tokens, 2 * tokens, None)
                    return inner

                lax.fori_loop(0, tokens // rows, tile, 0)

            @pl.when(i == j)
            def _():
                def tile(at, inner):
                    block, q_tile = at // (tokens // rows), at % (tokens // rows)
                    update(
                        i * tokens + q_tile * rows,
                        (2 * i + block) * tokens,
                        tokens,
                        q_tile * rows + (side - block) * tokens,
                    )
                    return inner

                lax.fori_loop(0, (side + 1) * (tokens // rows), tile, 0)

            @pl.when(word // 64 % 2 == 1)
            def _():
                result = kinds[kind]["result"]
                weight = lam[kind, level // 2]

                def finish(at, inner):
                    span = pl.ds(pl.multiple_of(i * tokens + at * rows, rows), rows)
                    first, second = (
                        acc[m, span, :value_size] / jnp.sum(total[m, span, :], axis=1, keepdims=True)
                        for m in range(2)
                    )
                    mixed = first - weight * second
                    result[span, :] = (
                        mixed * lax.rsqrt(jnp.mean(mixed * mixed, axis=1, keepdims=True) + 1e-06)
                    ).astype(result.dtype)
                    return inner

                lax.fori_loop(0, tokens // rows, finish, 0)
                for part in range(tp_count):
                    mine = jnp.logical_and(i == level, me_tp == part)
                    pl.when(mine)(lambda part=part: keep_result(kind, part).start())
                    pl.when(jnp.logical_not(mine))(lambda part=part: deliver(kind, i, part).start())

            return carry

        lax.fori_loop(0, steps, one_step, 0)

        for what in (1, 2):
            for at in range(levels):
                pl.when(level == at)(lambda what=what, at=at: across(kind, what, at, True).wait_send())
                pl.when(level != at)(lambda what=what, at=at: across(kind, what, at, False).wait_send())
        for i in range(levels):
            for part in range(tp_count):
                mine = jnp.logical_and(i == level, me_tp == part)
                pl.when(mine)(lambda part=part: keep_result(kind, part).wait())
                pl.when(jnp.logical_not(mine))(lambda i=i, part=part: deliver(kind, i, part).wait_send())

    of_kind(level, run)

    for which in range(2):
        share_shard(which, 1, peer, peer, False).wait_recv()
        shard_copy(which, 2).start()

    for rising, valid, one in over_targets((0, 1, 2), lambda copy: copy.wait_send()):
        pl.when(valid)(one)
    for origin in range(levels):
        for part in range(tp_count):
            kind = (origin + part) % 2
            ref = kinds[kind]["out"].at[:, column(kind, origin, part)]

            @pl.when(jnp.logical_not(jnp.logical_and(origin == level, part == me_tp)))
            def _(origin=origin, part=part, ref=ref):
                pltpu.make_async_remote_copy(
                    src_ref=ref, dst_ref=ref, send_sem=o_send.at[origin, part],
                    recv_sem=o_recv.at[origin, part], device_id=(2 * origin + side, part),
                    device_id_type=MESH,
                ).wait_recv()

    for which in range(2):
        keep_shard(which).wait()
        for at in range(3):
            shard_copy(which, at).wait_send()
        share_shard(which, 0, sibling, sibling, False).wait_recv()
        share_shard(which, 2, sibling, 2 * (1 - tp_y) + 1 - tp_core, False).wait_recv()

    width = stream.shape[1]
    step = math.gcd(width, 512)
    squares = jnp.zeros((share, 128), jnp.float32)

    def project(at, squares):
        span = pl.ds(pl.multiple_of(at * step, step), step)
        summed = jnp.dot(wide_out[...], pw[:, span], preferred_element_type=jnp.float32)
        summed = summed + jnp.dot(narrow_out[...], pn[:, span], preferred_element_type=jnp.float32)
        rounded = (summed + residual[:, span].astype(jnp.float32)).astype(stream.dtype)
        stream[:, span] = rounded
        value = rounded.astype(jnp.float32)
        square = value * value
        for piece in range(step // 128):
            squares = squares + square[:, piece * 128 : (piece + 1) * 128]
        return squares

    squares = lax.fori_loop(0, width // step, project, squares)
    factor = lax.rsqrt(jnp.sum(squares, axis=1, keepdims=True) / width + 1e-06)

    def normalize(at, carry):
        span = pl.ds(pl.multiple_of(at * step, step), step)
        normed[:, span] = (stream[:, span].astype(jnp.float32) * factor * gain[:, span]).astype(
            normed.dtype
        )
        return carry

    lax.fori_loop(0, width // step, normalize, 0)


def exchange_attention(
    lam, qw, kw, vw, qn, kn, vn, pw, pn, residual, gain, levels, tp_count, heads
):
    tokens = qw.shape[0]
    share = tokens // tp_count
    wide, narrow = [x.shape[1] // heads for x in (qw, kw, vw)], [x.shape[1] // heads for x in (qn, kn, vn)]
    most = max(wide[2], narrow[2])
    rows = levels * tokens

    def buffers(widths):
        return [
            pltpu.VMEM((rows, widths[0]), jnp.bfloat16),
            pltpu.VMEM((2 * rows, widths[1]), jnp.bfloat16),
            pltpu.VMEM((2 * rows, widths[2]), jnp.bfloat16),
        ]

    pairs = 2 * rows * rows * 2
    return pl.pallas_call(
        functools.partial(exchange_kernel, levels=levels, tp_count=tp_count, heads=heads),
        in_specs=[pl.BlockSpec(memory_space=pltpu.SMEM)] + [pl.BlockSpec(memory_space=pl.ANY)] * 8
        + [pl.BlockSpec(memory_space=pltpu.VMEM)] * 2,
        out_specs=[pl.BlockSpec(memory_space=pltpu.VMEM)] * 2,
        out_shape=[jax.ShapeDtypeStruct(residual.shape, jnp.bfloat16)] * 2,
        scratch_shapes=buffers(wide)
        + buffers(narrow)
        + [
            pltpu.VMEM((2, rows, most), jnp.float32),
            pltpu.VMEM((2, rows, 128), jnp.float32),
            pltpu.VMEM((2, rows, 128), jnp.float32),
            pltpu.VMEM((rows, wide[2]), jnp.bfloat16),
            pltpu.VMEM((rows, narrow[2]), jnp.bfloat16),
            pltpu.VMEM((share, tp_count * heads * wide[2]), jnp.bfloat16),
            pltpu.VMEM((share, tp_count * heads * narrow[2]), jnp.bfloat16),
            pltpu.VMEM((tp_count * pw.shape[0], pw.shape[1]), jnp.bfloat16),
            pltpu.VMEM((tp_count * pn.shape[0], pn.shape[1]), jnp.bfloat16),
            pltpu.SemaphoreType.DMA((6,)),
            pltpu.SemaphoreType.DMA((3, levels)),
            pltpu.SemaphoreType.DMA((3, levels)),
            pltpu.SemaphoreType.DMA((3, levels)),
            pltpu.SemaphoreType.DMA((3, levels)),
            pltpu.SemaphoreType.DMA((levels, tp_count)),
            pltpu.SemaphoreType.DMA((levels, tp_count)),
            pltpu.SemaphoreType.DMA((2, 3)),
            pltpu.SemaphoreType.DMA((2, 3)),
        ],
        compiler_params=pltpu.CompilerParams(
            vmem_limit_bytes=58 * 1024 * 1024, has_side_effects=True
        ),
        cost_estimate=pl.CostEstimate(
            flops=pairs * 1024, bytes_accessed=tokens * 4096 * 8, transcendentals=pairs
        ),
    )(lam, qw, kw, vw, qn, kn, vn, pw, pn, residual, gain)


def level_orders(levels):
    return [
        sorted(range(levels), key=lambda other: (abs(other - level), -other)) for level in range(levels)
    ]


def expert_kernel(
    outgoing, gate_in, up_in, down_in, returned,
    rows, gate, up, down, chosen, hidden, result, part, got_one, sum_one, got_two, final,
    own_sem, z_send, z_recv, y_send, y_recv, s_send, s_recv,
    one_send, one_recv, two_send, two_recv, back_send, back_recv,
    *, levels, slots, capacity,
):
    me_sp, me_tp = lax.axis_index("sp"), lax.axis_index("tp")
    level, side = me_sp // 2, me_sp % 2
    tp_y, tp_core = me_tp // 2, me_tp % 2
    sibling, peer = 2 * tp_y + 1 - tp_core, 2 * (1 - tp_y) + tp_core
    corner = 2 * (1 - tp_y) + 1 - tp_core
    width = returned.shape[1]
    group_rows, picked = GROUP * slots, GROUP * capacity
    orders = level_orders(levels)

    def pick_level(turn):
        return sum(
            jnp.where(jnp.logical_and(level == at, turn == place), orders[at][place], 0)
            for at in range(levels)
            for place in range(levels)
        )

    def span(index, size):
        return pl.ds(pl.multiple_of(index * size, size), size)

    def block(ref, origin, at_tp):
        return ref.at[span(origin * GROUP + at_tp, slots), :]

    def send(src, dst, send_sem, recv_sem, target):
        return pltpu.make_async_remote_copy(
            src_ref=src, dst_ref=dst, send_sem=send_sem, recv_sem=recv_sem,
            device_id=target, device_id_type=MESH,
        )

    def out_copy(target):
        return send(
            outgoing.at[span(target, slots), :], block(rows, me_sp, me_tp),
            z_send.at[target], z_recv.at[me_sp], (target, me_tp),
        )

    def out_keep():
        return pltpu.make_async_copy(
            outgoing.at[span(me_sp, slots), :], block(rows, me_sp, me_tp), own_sem.at[0]
        )

    def arrival(ref, sem, target):
        return send(ref, ref, z_send.at[0], sem, target)

    def y_copy(origin):
        ref = block(rows, origin, me_tp)
        return send(ref, ref, y_send.at[origin], y_recv.at[origin], (me_sp, peer))

    def s_copy(origin, which):
        ref = block(rows, origin, peer if which else me_tp)
        return send(ref, ref, s_send.at[origin, which], s_recv.at[origin, which], (me_sp, sibling))

    def one_copy(origin, half):
        return send(
            block(part, origin, 2 * half + 1 - tp_core), got_one.at[span(2 * origin + half, slots), :],
            one_send.at[origin, half], one_recv.at[origin, half], (me_sp, sibling),
        )

    def two_copy(origin):
        return send(
            sum_one.at[span(origin, slots), :], got_two.at[span(origin, slots), :],
            two_send.at[origin], two_recv.at[origin], (me_sp, peer),
        )

    def back_copy(origin):
        return send(
            final.at[span(origin, slots), :], returned.at[span(me_sp, slots), :],
            back_send.at[origin], back_recv.at[me_sp], (origin, me_tp),
        )

    weights = [
        pltpu.make_async_copy(src, dst, own_sem.at[1 + at])
        for at, (src, dst) in enumerate(((gate_in, gate), (up_in, up), (down_in, down)))
    ]
    out_keep().start()
    for turn in range(levels):
        there = pick_level(turn)
        for other in range(2):
            if turn == 0 and other == 0:
                continue
            out_copy(2 * there + (side + other) % 2).start()
    for copy in weights:
        copy.start()

    def both(turn, body):
        there = pick_level(turn)
        for other in range(2):
            body(2 * there + (side + other) % 2, other)

    def spread(origin, other):
        pl.when(origin == me_sp)(lambda: out_keep().wait())
        pl.when(origin != me_sp)(
            lambda: arrival(block(rows, origin, me_tp), z_recv.at[origin], (me_sp, peer)).wait_recv()
        )
        y_copy(origin).start()
        s_copy(origin, 0).start()

    def pass_on(origin, other):
        arrival(block(rows, origin, peer), y_recv.at[origin], (me_sp, peer)).wait_recv()
        s_copy(origin, 1).start()

    def selection(origin):
        notes = rows[span(origin, group_rows), width:].astype(jnp.float32)
        lane = lax.broadcasted_iota(jnp.int32, notes.shape, 1)
        rank = jnp.sum(jnp.where(lane == me_tp, notes, 0.0), axis=1, keepdims=True)
        share = jnp.sum(
            jnp.where(jnp.logical_and(lane >= GROUP, lane % GROUP == me_tp), notes, 0.0),
            axis=1, keepdims=True,
        )
        at_row = lax.broadcasted_iota(jnp.int32, (group_rows, picked), 0)
        at_col = lax.broadcasted_iota(jnp.int32, (group_rows, picked), 1)
        wanted = (at_col - at_row // slots * capacity + 1).astype(jnp.float32)
        hit = jnp.logical_and(wanted == rank, rank > 0.5)
        return hit.astype(jnp.float32).astype(jnp.bfloat16), share

    def choose(origin, other):
        arrival(block(rows, origin, sibling), s_recv.at[origin, 0], (me_sp, sibling)).wait_recv()
        arrival(block(rows, origin, corner), s_recv.at[origin, 1], (me_sp, sibling)).wait_recv()
        table, _ = selection(origin)
        chosen[other * picked : (other + 1) * picked, :] = lax.dot_general(
            table, rows[span(origin, group_rows), :width], (((0,), (0,)), ((), ())),
            preferred_element_type=jnp.float32,
        ).astype(jnp.bfloat16)

    def experts():
        tile = math.gcd(hidden.shape[1], 256)

        def inner(at, carry):
            cols = span(at, tile)
            gated = jnp.dot(chosen[...], gate[:, cols], preferred_element_type=jnp.float32)
            lifted = jnp.dot(chosen[...], up[:, cols], preferred_element_type=jnp.float32)
            hidden[:, cols] = (gated / (1.0 + jnp.exp(-gated)) * lifted).astype(jnp.bfloat16)
            return carry

        lax.fori_loop(0, hidden.shape[1] // tile, inner, 0)
        wide = math.gcd(width, 512)

        def outer(at, carry):
            cols = span(at, wide)
            result[:, cols] = jnp.dot(
                hidden[...], down[:, cols], preferred_element_type=jnp.float32
            ).astype(jnp.bfloat16)
            return carry

        lax.fori_loop(0, width // wide, outer, 0)

    def spread_result(origin, other):
        table, share = selection(origin)
        wide = math.gcd(width, 512)
        for at in range(width // wide):
            cols = slice(at * wide, (at + 1) * wide)
            placed = jnp.dot(
                table, result[other * picked : (other + 1) * picked, cols],
                preferred_element_type=jnp.float32,
            )
            part[span(origin, group_rows), cols] = (share * placed).astype(jnp.bfloat16)
        for half in range(2):
            one_copy(origin, half).start()

    def add_one(origin, other):
        for half in range(2):
            arrival(
                got_one.at[span(2 * origin + half, slots), :], one_recv.at[origin, half], (me_sp, sibling)
            ).wait_recv()
        away = 1 - tp_y
        mine = part[span(origin * GROUP + 2 * away + tp_core, slots), :].astype(jnp.float32)
        theirs = got_one[span(2 * origin + away, slots), :].astype(jnp.float32)
        sum_one[span(origin, slots), :] = (mine + theirs).astype(jnp.bfloat16)
        two_copy(origin).start()

    def add_two(origin, other):
        arrival(got_two.at[span(origin, slots), :], two_recv.at[origin], (me_sp, peer)).wait_recv()
        mine = part[span(origin * GROUP + me_tp, slots), :].astype(jnp.float32)
        theirs = got_one[span(2 * origin + tp_y, slots), :].astype(jnp.float32)
        summed = mine + theirs + got_two[span(origin, slots), :].astype(jnp.float32)
        final[span(origin, slots), :] = summed.astype(jnp.bfloat16)
        pl.when(origin != me_sp)(lambda: back_copy(origin).start())

        @pl.when(origin == me_sp)
        def _():
            returned[span(me_sp, slots), :] = summed.astype(jnp.bfloat16)

    def turn_body(turn, carry):
        @pl.when(turn < levels)
        def _():
            both(turn, spread)

        @pl.when(turn == 1)
        def _():
            for copy in weights:
                copy.wait()

        @pl.when(jnp.logical_and(turn >= 1, turn <= levels))
        def _():
            both(turn - 1, choose)
            experts()
            both(turn - 1, spread_result)

        @pl.when(turn < levels)
        def _():
            both(turn, pass_on)

        @pl.when(jnp.logical_and(turn >= 1, turn <= levels))
        def _():
            both(turn - 1, add_one)

        @pl.when(turn >= 2)
        def _():
            both(turn - 2, add_two)

        return carry

    lax.fori_loop(0, levels + 2, turn_body, 0)

    def drain(origin, carry):
        @pl.when(origin != me_sp)
        def _():
            out_copy(origin).wait_send()
            back_copy(origin).wait_send()
            arrival(
                returned.at[span(origin, slots), :], back_recv.at[origin], (origin, me_tp)
            ).wait_recv()

        y_copy(origin).wait_send()
        two_copy(origin).wait_send()
        for which in range(2):
            s_copy(origin, which).wait_send()
            one_copy(origin, which).wait_send()
        return carry

    lax.fori_loop(0, 2 * levels, drain, 0)


def grouped_experts(
    stream, normed, expert_ids, expert_weights, gate, up, down, sp_size, tp_size
):
    local_rows, width = normed.shape
    experts_all = sp_size * tp_size
    capacity = max(2, 4 * local_rows // experts_all)
    slots = GROUP * capacity // 2
    in_group = expert_ids % GROUP
    group = expert_ids[:, 0] // GROUP
    earlier = jnp.tri(local_rows, k=-1, dtype=jnp.bfloat16)
    group_hot = group[:, None] == jnp.arange(sp_size, dtype=jnp.int32)[None, :]
    expert_hot = jnp.any(
        expert_ids[:, :, None] == jnp.arange(experts_all, dtype=jnp.int32)[None, None, :], axis=1
    )
    hot = jnp.concatenate([group_hot, expert_hot], axis=1)
    before = jnp.dot(earlier, hot.astype(jnp.bfloat16), preferred_element_type=jnp.float32)
    group_rank = jnp.sum(jnp.where(group_hot, before[:, :sp_size], 0.0), axis=1).astype(jnp.int32)
    slot = group * slots + group_rank
    rank = jnp.where(expert_hot, before[:, sp_size:] + 1.0, 0.0)
    rank = jnp.sum(rank.reshape(local_rows, sp_size, GROUP), axis=1)
    share = jnp.sum(
        jnp.where(
            in_group[:, :, None] == jnp.arange(GROUP, dtype=jnp.int32)[None, None, :],
            expert_weights[:, :, None], 0.0,
        ),
        axis=1,
    )
    high = lax.reduce_precision(share, 8, 7)
    middle = lax.reduce_precision(share - high, 8, 7)
    low = share - high - middle
    notes = jnp.concatenate([rank, high, middle, low], axis=1).astype(jnp.bfloat16)
    notes = jnp.pad(notes, ((0, 0), (0, 128 - 4 * GROUP)))
    place = (
        slot[:, None] == jnp.arange(sp_size * slots, dtype=jnp.int32)[None, :]
    ).astype(jnp.bfloat16)
    outgoing = lax.dot_general(
        place, jnp.concatenate([normed, notes], axis=1), (((0,), (0,)), ((), ())),
        preferred_element_type=jnp.float32,
    ).astype(jnp.bfloat16)

    levels = sp_size // 2
    every = sp_size * GROUP * slots
    own = sp_size * slots
    picked = 2 * GROUP * capacity
    hidden_size = gate.shape[1]
    dma = pltpu.SemaphoreType.DMA
    returned = pl.pallas_call(
        functools.partial(expert_kernel, levels=levels, slots=slots, capacity=capacity),
        in_specs=[pl.BlockSpec(memory_space=pl.ANY)] * 4,
        out_specs=pl.BlockSpec(memory_space=pltpu.VMEM),
        out_shape=jax.ShapeDtypeStruct((own, width), jnp.bfloat16),
        scratch_shapes=[
            pltpu.VMEM((every, outgoing.shape[1]), jnp.bfloat16),
            pltpu.VMEM(gate.shape, jnp.bfloat16),
            pltpu.VMEM(up.shape, jnp.bfloat16),
            pltpu.VMEM(down.shape, jnp.bfloat16),
            pltpu.VMEM((picked, width), jnp.bfloat16),
            pltpu.VMEM((picked, hidden_size), jnp.bfloat16),
            pltpu.VMEM((picked, width), jnp.bfloat16),
            pltpu.VMEM((every, width), jnp.bfloat16),
            pltpu.VMEM((2 * own, width), jnp.bfloat16),
            pltpu.VMEM((own, width), jnp.bfloat16),
            pltpu.VMEM((own, width), jnp.bfloat16),
            pltpu.VMEM((own, width), jnp.bfloat16),
            dma((4,)),
        ]
        + [dma((sp_size,))] * 4
        + [dma((sp_size, 2))] * 4
        + [dma((sp_size,))] * 4,
        compiler_params=pltpu.CompilerParams(
            vmem_limit_bytes=58 * 1024 * 1024, has_side_effects=True
        ),
        cost_estimate=pl.CostEstimate(
            flops=6 * own * width * hidden_size * 2,
            bytes_accessed=6 * width * hidden_size,
            transcendentals=own * hidden_size,
        ),
    )(outgoing, gate, up, down)
    summed = jnp.dot(place, returned, preferred_element_type=jnp.float32)
    return (stream.astype(jnp.float32) + summed).astype(jnp.bfloat16)


def ring_order(count):
    return list(range(0, count, 2)) + list(range(1, count, 2))[::-1]


def ring_attention(
    query_wide, key_wide, value_wide, query_narrow, key_narrow, value_narrow, mix_lambda
):
    tok_count, local_heads, _ = query_wide.shape
    size_wide = query_wide.shape[2] // 2
    size_narrow = query_narrow.shape[2] // 2

    value_wide_size, value_narrow_size = value_wide.shape[2], value_narrow.shape[2]
    flat = lambda member: member.reshape(tok_count, -1)
    own = jnp.concatenate(
        [flat(key_wide), flat(value_wide), flat(key_narrow), flat(value_narrow)], axis=1
    )
    wide_q, narrow_q = flat(query_wide), flat(query_narrow)
    wide_v_col = local_heads * 2 * size_wide
    narrow_k_col = wide_v_col + local_heads * value_wide_size
    narrow_v_col = narrow_k_col + local_heads * 2 * size_narrow

    count = lax.axis_size("sp")
    order = ring_order(count)
    place = [order.index(device) for device in range(count)]
    me = lax.axis_index("sp")
    order_table = jnp.array(order, jnp.int32)
    my_place = jnp.array(place, jnp.int32)[me]
    forward = [(order[i], order[(i + 1) % count]) for i in range(count)]
    backward = [(b, a) for a, b in forward]

    def source_flag(shift):
        return (order_table[(my_place + shift) % count] < me).astype(jnp.int32)

    def both(pieces, flags, states, final=False):
        return (
            attend(
                wide_q, pieces, flags, states[0], mix_lambda[0], size_wide, value_wide_size,
                0, wide_v_col, final,
            ),
            attend(
                narrow_q, pieces, flags, states[1], mix_lambda[1], size_narrow, value_narrow_size,
                narrow_k_col, narrow_v_col, final,
            ),
        )

    half = tok_count // 2
    pieces = [(own, 0, tok_count)]
    flags = jnp.ones((2,), jnp.int32)
    states = (None, None)
    left = right = own
    for step in range(1, count // 2 + 1):
        if step < count // 2:
            left = lax.ppermute(left, "sp", forward)
            right = lax.ppermute(right, "sp", backward)
            coming = [(left, 0, tok_count), (right, 0, tok_count)]
        else:
            coming = [
                (lax.ppermute(left[:half], "sp", forward), 0, half),
                (lax.ppermute(right[half:], "sp", backward), 0, half),
            ]
        states = both(pieces, flags, states)
        arrived_now, states = lax.optimization_barrier(
            (tuple(piece for piece, _, _ in coming), states)
        )
        pieces = [(arrived_now[i], 0, coming[i][2]) for i in range(2)]
        left, right = arrived_now
        flags = jnp.stack([source_flag(-step), source_flag(step)])
    heads_wide, heads_narrow = both(pieces, flags, states, final=True)
    return (
        lax.all_to_all(heads_wide, "tp", split_axis=0, concat_axis=1, tiled=True),
        lax.all_to_all(heads_narrow, "tp", split_axis=0, concat_axis=1, tiled=True),
    )


def shards(
    query_wide,
    key_wide,
    value_wide,
    query_narrow,
    key_narrow,
    value_narrow,
    mix_lambda,
    residual_in,
    out_wide,
    out_narrow,
    ffn_gain,
    expert_ids,
    expert_weights,
    gate_weight,
    up_weight,
    down_weight,
):
    tok_count, local_heads, _ = query_wide.shape
    tp_size, sp_size = lax.axis_size("tp"), lax.axis_size("sp")
    local_rows = tok_count // tp_size
    attention_args = (
        query_wide, key_wide, value_wide, query_narrow, key_narrow, value_narrow, mix_lambda
    )
    fits = sp_size == 8 and local_heads * 4 == sp_size and tp_size == GROUP
    if fits:
        flat = [member.reshape(tok_count, -1) for member in attention_args[:6]]
        stream, normed = exchange_attention(
            mix_lambda, *flat, out_wide, out_narrow, residual_in, ffn_gain[None, :],
            sp_size // 2, tp_size, local_heads,
        )
        return grouped_experts(
            stream, normed, expert_ids, expert_weights, gate_weight[0], up_weight[0],
            down_weight[0], sp_size, tp_size,
        )
    mine_wide, mine_narrow = ring_attention(*attention_args)
    whole_wide, whole_narrow = (
        lax.all_gather(out_wide, "tp", axis=0, tiled=True),
        lax.all_gather(out_narrow, "tp", axis=0, tiled=True),
    )
    projected = jnp.dot(mine_wide, whole_wide, preferred_element_type=jnp.float32) + jnp.dot(
        mine_narrow, whole_narrow, preferred_element_type=jnp.float32
    )
    stream = (projected + residual_in.astype(jnp.float32)).astype(jnp.bfloat16)
    stream_f = stream.astype(jnp.float32)
    normed = (
        stream_f
        * lax.rsqrt(jnp.mean(stream_f * stream_f, axis=-1, keepdims=True) + 1e-06)
        * ffn_gain
    ).astype(jnp.bfloat16)
    experts_all = lax.axis_size("sp") * tp_size
    capacity = max(2, 4 * local_rows // experts_all)
    model_width = normed.shape[1]
    flat_expert = expert_ids.reshape(-1)
    expert_hot = (flat_expert[:, None] == jnp.arange(experts_all, dtype=jnp.int32)[None, :]).astype(
        jnp.int32
    )
    slot_rank = jnp.sum((jnp.cumsum(expert_hot, axis=0) - 1) * expert_hot, axis=1)
    flat_slot = flat_expert * capacity + slot_rank
    slot_ids = jnp.arange(experts_all * capacity, dtype=jnp.int32)
    placed = slot_ids[:, None] == flat_slot[None, :]
    dispatch = jnp.any(placed.reshape(experts_all * capacity, local_rows, 2), axis=2).astype(
        jnp.bfloat16
    )
    outgoing = jnp.dot(dispatch, normed, preferred_element_type=jnp.float32).astype(jnp.bfloat16)
    outgoing = outgoing.reshape(experts_all, capacity, model_width)
    arrived = lax.all_to_all(outgoing, ("sp", "tp"), split_axis=0, concat_axis=0, tiled=True)
    sources, items, width = arrived.shape
    flat_rows = arrived.reshape(sources * items, width)
    gate_part = jnp.dot(flat_rows, gate_weight[0], preferred_element_type=jnp.float32)
    up_part = jnp.dot(flat_rows, up_weight[0], preferred_element_type=jnp.float32)
    hidden = (jax.nn.silu(gate_part) * up_part).astype(jnp.bfloat16)
    result = jnp.dot(hidden, down_weight[0], preferred_element_type=jnp.float32).astype(
        jnp.bfloat16
    )
    returned = lax.all_to_all(
        result.reshape(sources, items, width), ("sp", "tp"), split_axis=0, concat_axis=0, tiled=True
    )
    slot_hot = (flat_slot[:, None] == slot_ids[None, :]).astype(
        jnp.float32
    ) * expert_weights.reshape(-1)[:, None]
    combine = jnp.sum(slot_hot.reshape(local_rows, 2, experts_all * capacity), axis=1)
    summed = jnp.dot(
        combine,
        returned.reshape(experts_all * capacity, model_width).astype(jnp.float32),
        precision=lax.Precision.HIGHEST,
    )
    return (stream_f + summed).astype(jnp.bfloat16)


def solution(mesh):
    return jax.shard_map(
        shards,
        mesh=mesh,
        in_specs=(
            P("sp", "tp", None),
            P("sp", "tp", None),
            P("sp", "tp", None),
            P("sp", "tp", None),
            P("sp", "tp", None),
            P("sp", "tp", None),
            P(None, "tp"),
            P(("sp", "tp"), None),
            P("tp", None),
            P("tp", None),
            P(),
            P(("sp", "tp"), None),
            P(("sp", "tp"), None),
            P(("sp", "tp"), None, None),
            P(("sp", "tp"), None, None),
            P(("sp", "tp"), None, None),
        ),
        out_specs=P(("sp", "tp"), None),
        check_vma=False,
    )
```

```python
import functools
import math

import jax
import jax.numpy as jnp
from jax import lax
from jax.experimental import pallas as pl
from jax.experimental.pallas import tpu as pltpu
from jax.sharding import PartitionSpec as P

NEG_FILL = -1e30
GROUP = 4


def attend_kernel(flags, lam, *refs, count, diag, final, head_size, packed):
    q_ref = refs[0]
    blocks = [(refs[1 + 2 * b], refs[2 + 2 * b]) for b in range(count)]
    refs = refs[1 + 2 * count :]
    if not diag:
        acc_in, stat_in = refs[:2]
        refs = refs[2:]
    if final:
        out_ref, acc, peak, total = refs
    else:
        acc_out, stat_out, acc, peak, total = refs
    scale = head_size ** (-0.5) * math.log2(math.e)
    rows = q_ref.shape[0]
    head = pl.program_id(0)
    first_row = pl.program_id(1) * rows

    def lanes(column):
        return jnp.broadcast_to(column, (rows, 128))

    if not diag:
        acc[...] = acc_in[...]
        for m in range(2):
            peak[m] = lanes(stat_in[0, :, 2 * m : 2 * m + 1])
            total[m] = lanes(stat_in[0, :, 2 * m + 1 : 2 * m + 2])

    def update(k_ref, v_ref):
        values = v_ref[...]
        for m in range(2):
            if packed:
                side = lax.broadcasted_iota(jnp.int32, q_ref.shape, 1) // head_size
                query = jnp.where(side == m, q_ref[...], jnp.zeros_like(q_ref))
                keys = k_ref[...]
            else:
                query = q_ref[:, m * head_size : (m + 1) * head_size]
                keys = k_ref[:, m * head_size : (m + 1) * head_size]
            scores = (
                lax.dot_general(
                    query, keys, (((1,), (1,)), ((), ())), preferred_element_type=jnp.float32
                )
                * scale
            )
            if diag:
                row = first_row + lax.broadcasted_iota(jnp.int32, scores.shape, 0)
                col = lax.broadcasted_iota(jnp.int32, scores.shape, 1)
                scores = jnp.where(col <= row, scores, NEG_FILL)
            new_peak = jnp.max(scores, axis=1, keepdims=True)
            if not diag:
                old_peak = peak[m][:, :1]
                new_peak = jnp.maximum(old_peak, new_peak)
                factor = jnp.exp2(old_peak - new_peak)
            weights = jnp.exp2(scores - new_peak)
            new_total = jnp.sum(weights, axis=1, keepdims=True)
            read = jnp.dot(
                weights.astype(jnp.bfloat16), values, preferred_element_type=jnp.float32
            )
            if not diag:
                new_total = new_total + factor * total[m][:, :1]
                read = read + factor * acc[m]
            acc[m] = read
            peak[m] = lanes(new_peak)
            total[m] = lanes(new_total)

    for b in range(count):
        if diag:
            update(*blocks[b])
        else:
            pl.when(flags[b] == 1)(functools.partial(update, *blocks[b]))

    if final:
        mixed = acc[0] / total[0][:, :1] - lam[head] * (acc[1] / total[1][:, :1])
        out_ref[...] = (
            mixed * lax.rsqrt(jnp.mean(mixed * mixed, axis=1, keepdims=True) + 1e-06)
        ).astype(out_ref.dtype)
    else:
        acc_out[...] = acc[...]
        lane = lax.broadcasted_iota(jnp.int32, (rows, 128), 1)
        stat_out[0] = jnp.where(
            lane == 0,
            peak[0],
            jnp.where(lane == 1, total[0], jnp.where(lane == 2, peak[1], total[1])),
        )


def attend(query, pieces, flags, state, lam, head_size, value_size, key_col, value_col, final):
    diag = state is None
    tok_count, width = query.shape
    heads = width // (2 * head_size)
    block = math.gcd(tok_count, 256)
    packed = head_size % 128 != 0
    kb, vb = key_col // (2 * head_size), value_col // value_size
    q_spec = pl.BlockSpec((block, 2 * head_size), lambda h, i, *_: (i, h))
    acc_spec = pl.BlockSpec((2, block, value_size), lambda h, i, *_: (0, i, h))
    stat_spec = pl.BlockSpec((1, block, 128), lambda h, i, *_: (h, i, 0))
    in_specs, operands = [q_spec], [query]
    keys_seen = 0
    for piece, start, rows in pieces:
        keys_seen += rows
        at = start // rows
        in_specs += [
            pl.BlockSpec((rows, 2 * head_size), lambda h, i, *_, at=at: (at, kb + h)),
            pl.BlockSpec((rows, value_size), lambda h, i, *_, at=at: (at, vb + h)),
        ]
        operands += [piece, piece]
    aliases = {}
    if not diag:
        in_specs += [acc_spec, stat_spec]
        operands += list(state)
        if not final:
            aliases = {2 + len(operands) - 2: 0, 2 + len(operands) - 1: 1}
    if final:
        out_specs = pl.BlockSpec((block, value_size), lambda h, i, *_: (i, h))
        out_shape = jax.ShapeDtypeStruct((tok_count, heads * value_size), jnp.bfloat16)
    else:
        out_specs = (acc_spec, stat_spec)
        out_shape = (
            jax.ShapeDtypeStruct((2, tok_count, heads * value_size), jnp.float32),
            jax.ShapeDtypeStruct((heads, tok_count, 128), jnp.float32),
        )
    pairs = heads * tok_count * keys_seen * 2
    return pl.pallas_call(
        functools.partial(
            attend_kernel,
            count=len(pieces),
            diag=diag,
            final=final,
            head_size=head_size,
            packed=packed,
        ),
        grid_spec=pltpu.PrefetchScalarGridSpec(
            num_scalar_prefetch=2,
            grid=(heads, tok_count // block),
            in_specs=in_specs,
            out_specs=out_specs,
            scratch_shapes=[
                pltpu.VMEM((2, block, value_size), jnp.float32),
                pltpu.VMEM((2, block, 128), jnp.float32),
                pltpu.VMEM((2, block, 128), jnp.float32),
            ],
        ),
        out_shape=out_shape,
        input_output_aliases=aliases,
        compiler_params=pltpu.CompilerParams(vmem_limit_bytes=40 * 1024 * 1024),
        cost_estimate=pl.CostEstimate(
            flops=pairs * 1024,
            bytes_accessed=keys_seen * heads * (2 * head_size + value_size) * 2
            + tok_count * heads * value_size * 16,
            transcendentals=pairs,
        ),
    )(flags, lam, *operands)


MESH = pl.DeviceIdType.MESH


def pair_tables():
    orders = (
        ((0, 0), (1, 0), (2, 0), (3, 0), (1, 1), (2, 1), (3, 1), (2, 2), (3, 2), (3, 3)),
        ((1, 1), (2, 1), (1, 0), (2, 0), (3, 1), (3, 0), (0, 0), (2, 2), (3, 2), (3, 3)),
        ((2, 2), (3, 2), (2, 1), (3, 1), (2, 0), (3, 0), (3, 3), (1, 1), (1, 0), (0, 0)),
        ((3, 3), (3, 2), (3, 1), (3, 0), (2, 2), (2, 1), (2, 0), (1, 1), (1, 0), (0, 0)),
    )
    passing = ({2: 1, 6: 2, 8: 3}, {1: 0, 5: 2, 8: 3}, {1: 1, 3: 0, 5: 3}, {1: 2, 2: 1, 3: 0})
    words = []
    for level, order in enumerate(orders):
        row, seen_q, seen_k = [], {level}, set()
        for at, (i, j) in enumerate(order):
            word = i + 4 * j
            if i not in seen_q:
                word += 16
            if j not in seen_k:
                word += 32
            if all(pair[0] != i for pair in order[at + 1 :]):
                word += 64
            word += 128 * (passing[level][at] + 1 if at in passing[level] else 0)
            seen_q.add(i)
            seen_k.add(j)
            row.append(word)
        words.append(row)
    return words


def route(ids, shares, place, notes, groups, slots):
    count = ids.shape[1]
    bits = GROUP.bit_length() - 1
    group = [ids[at : at + 1, :] >> bits for at in range(2)]
    inner = [ids[at : at + 1, :] - (group[at] << bits) for at in range(2)]

    def rows_of(size):
        return lax.broadcasted_iota(jnp.int32, (size, count), 0)

    def as_number(hit):
        return hit.astype(jnp.float32)

    earlier = as_number(
        lax.broadcasted_iota(jnp.int32, (count, count), 0)
        < lax.broadcasted_iota(jnp.int32, (count, count), 1)
    ).astype(jnp.bfloat16)

    def before(hot):
        return jnp.dot(hot.astype(jnp.bfloat16), earlier, preferred_element_type=jnp.float32)

    group_hot = as_number(rows_of(groups) == group[0])
    expert_row = rows_of(groups * GROUP)
    expert_hot = as_number(jnp.logical_or(expert_row == ids[0:1, :], expert_row == ids[1:2, :]))
    group_rank = jnp.sum(group_hot * before(group_hot), axis=0, keepdims=True)
    slot = group[0] * slots + group_rank.astype(jnp.int32)
    place[...] = as_number(rows_of(groups * slots) == slot).astype(place.dtype)
    expert_rank = expert_hot * (before(expert_hot) + 1.0)
    at_row = rows_of(notes.shape[0])
    table = jnp.zeros(notes.shape, jnp.float32)
    for k in range(GROUP):
        rank = jnp.sum(
            jnp.where(expert_row & (GROUP - 1) == k, expert_rank, 0.0), axis=0, keepdims=True
        )
        share = sum(jnp.where(inner[at] == k, shares[at : at + 1, :], 0.0) for at in range(2))
        high = share.astype(jnp.bfloat16).astype(jnp.float32)
        middle = (share - high).astype(jnp.bfloat16).astype(jnp.float32)
        for piece, value in enumerate((rank, high, middle, share - high - middle)):
            table = jnp.where(at_row == piece * GROUP + k, value, table)
    notes[...] = table.astype(notes.dtype)


def exchange_kernel(
    lam, qw_in, kw_in, vw_in, qn_in, kn_in, vn_in, pw_in, pn_in, residual, gain, ids, shares,
    stream, outgoing, place,
    qw, kw, vw, qn, kn, vn, acc, peak, total, ow, on, wide_out, narrow_out, pw, pn,
    normed, notes,
    own_sem, z_send, z_recv, x_send, x_recv, o_send, o_recv, p_send, p_recv,
    *, levels, tp_count, heads,
):
    me_sp, me_tp = lax.axis_index("sp"), lax.axis_index("tp")
    level, side = me_sp // 2, me_sp % 2
    flavour = me_tp % 2
    tokens = qw_in.shape[0]
    share = tokens // tp_count
    kinds = (
        dict(ins=(qw_in, kw_in, vw_in), bufs=(qw, kw, vw), result=ow, out=wide_out),
        dict(ins=(qn_in, kn_in, vn_in), bufs=(qn, kn, vn), result=on, out=narrow_out),
    )
    for entry in kinds:
        entry["widths"] = tuple(ref.shape[1] // heads for ref in entry["ins"])

    def source(kind, what, head):
        width = kinds[kind]["widths"][what]
        return kinds[kind]["ins"][what].at[:, pl.ds(pl.multiple_of(head * width, width), width)]

    def slot(kind, what, at, other):
        block = at if what == 0 else 2 * at + other
        return kinds[kind]["bufs"][what].at[pl.ds(pl.multiple_of(block * tokens, tokens), tokens), :]

    def to_level(kind, what, target):
        return pltpu.make_async_remote_copy(
            src_ref=source(kind, what, target // 2),
            dst_ref=slot(kind, what, level, side),
            send_sem=z_send.at[what, target],
            recv_sem=z_recv.at[what, level],
            device_id=(2 * target + side, me_tp),
            device_id_type=MESH,
        )

    def from_level(kind, what, origin):
        ref = slot(kind, what, origin, side)
        return pltpu.make_async_remote_copy(
            src_ref=ref, dst_ref=ref, send_sem=z_send.at[what, origin],
            recv_sem=z_recv.at[what, origin], device_id=(2 * origin + side, me_tp), device_id_type=MESH,
        )

    def across(kind, what, at, own):
        return pltpu.make_async_remote_copy(
            src_ref=source(kind, what, level // 2) if own else slot(kind, what, at, side),
            dst_ref=slot(kind, what, at, side),
            send_sem=x_send.at[what, at],
            recv_sem=x_recv.at[what, at],
            device_id=(2 * level + 1 - side, me_tp),
            device_id_type=MESH,
        )

    def from_across(kind, what, at):
        ref = slot(kind, what, at, 1 - side)
        return pltpu.make_async_remote_copy(
            src_ref=ref, dst_ref=ref, send_sem=x_send.at[what, at], recv_sem=x_recv.at[what, at],
            device_id=(2 * level + 1 - side, me_tp), device_id_type=MESH,
        )

    def keep(kind, what):
        return pltpu.make_async_copy(
            source(kind, what, level // 2), slot(kind, what, level, side), own_sem.at[what]
        )

    def column(kind, at_level, at_tp):
        width = kinds[kind]["widths"][2]
        return pl.ds(pl.multiple_of((at_tp * heads + at_level // 2) * width, width), width)

    def result_rows(kind, i, part):
        return kinds[kind]["result"].at[
            pl.ds(pl.multiple_of(i * tokens + part * share, share), share), :
        ]

    def deliver(kind, i, part):
        return pltpu.make_async_remote_copy(
            src_ref=result_rows(kind, i, part),
            dst_ref=kinds[kind]["out"].at[:, column(kind, level, me_tp)],
            send_sem=o_send.at[i, part],
            recv_sem=o_recv.at[level, me_tp],
            device_id=(2 * i + side, part),
            device_id_type=MESH,
        )

    def keep_result(kind, part):
        return pltpu.make_async_copy(
            result_rows(kind, level, part),
            kinds[kind]["out"].at[:, column(kind, level, me_tp)],
            own_sem.at[3],
        )

    def of_kind(at_level, body):
        kind_here = (at_level + flavour) % 2
        for kind in range(2):
            pl.when(kind_here == kind)(functools.partial(body, kind))

    def begin_own(kind):
        for what in (1, 2):
            across(kind, what, level, True).start()
        for what in range(3):
            keep(kind, what).start()

    of_kind(level, begin_own)

    tp_y, tp_core = me_tp // 2, me_tp % 2
    sibling, peer = 2 * tp_y + 1 - tp_core, 2 * (1 - tp_y) + tp_core
    projections = ((pw_in, pw), (pn_in, pn))

    def shard_of(which, at_tp):
        rows = projections[which][0].shape[0]
        return projections[which][1].at[pl.ds(pl.multiple_of(at_tp * rows, rows), rows), :]

    def share_shard(which, at, target, owner, own):
        return pltpu.make_async_remote_copy(
            src_ref=projections[which][0] if own else shard_of(which, owner),
            dst_ref=shard_of(which, owner),
            send_sem=p_send.at[which, at],
            recv_sem=p_recv.at[which, at],
            device_id=(me_sp, target),
            device_id_type=MESH,
        )

    def keep_shard(which):
        return pltpu.make_async_copy(
            projections[which][0], shard_of(which, me_tp), own_sem.at[4 + which]
        )

    def shard_copy(which, at):
        if at == 2:
            return share_shard(which, 2, sibling, peer, False)
        return share_shard(which, at, (sibling, peer)[at], me_tp, True)

    for which in range(2):
        keep_shard(which).start()
        for at in range(2):
            shard_copy(which, at).start()

    def over_targets(whats, body):
        for step in range(1, levels):
            for target in (level + step, level - step):
                rising = target > level

                def one(target=target):
                    def at_kind(kind):
                        for what in whats:
                            body(to_level(kind, what, target))

                    of_kind(target, at_kind)

                yield rising, jnp.logical_and(target >= 0, target < levels), one

    early_up = list(over_targets((1, 2), lambda copy: copy.start()))
    early_down = list(over_targets((0,), lambda copy: copy.start()))
    for rising, valid, one in early_up:
        pl.when(jnp.logical_and(valid, rising))(one)
    for rising, valid, one in early_down:
        pl.when(jnp.logical_and(valid, jnp.logical_not(rising)))(one)
    for rising, valid, one in early_up:
        pl.when(jnp.logical_and(valid, jnp.logical_not(rising)))(one)
    for rising, valid, one in early_down:
        pl.when(jnp.logical_and(valid, rising))(one)

    words = pair_tables()
    steps = len(words[0])
    here = [
        sum(jnp.where(level == at, words[at][step], 0) for at in range(levels)) for step in range(steps)
    ]

    def run(kind):
        q_buf, k_buf, v_buf = kinds[kind]["bufs"]
        head_size = q_buf.shape[1] // 2
        value_size = v_buf.shape[1]
        packed = head_size % 128 != 0
        scale = head_size ** (-0.5) * math.log2(math.e)
        rows = tokens // tp_count * (tp_count // 2)

        def clear(at, carry):
            span = pl.ds(pl.multiple_of(at * rows, rows), rows)
            for m in range(2):
                acc[m, span, :value_size] = jnp.zeros((rows, value_size), jnp.float32)
                peak[m, span, :] = jnp.full((rows, 128), NEG_FILL, jnp.float32)
                total[m, span, :] = jnp.zeros((rows, 128), jnp.float32)
            return carry

        lax.fori_loop(0, levels * tokens // rows, clear, 0)
        for what in range(3):
            keep(kind, what).wait()

        def update(q_at, k_at, count, edge):
            q_span = pl.ds(pl.multiple_of(q_at, rows), rows)
            k_span = pl.ds(pl.multiple_of(k_at, tokens), count)
            values = v_buf[k_span, :]
            found = []
            for m in range(2):
                if packed:
                    query, keys = q_buf[q_span, :], k_buf[k_span, :]
                    half = lax.broadcasted_iota(jnp.int32, query.shape, 1) // head_size
                    query = jnp.where(half == m, query, jnp.zeros_like(query))
                else:
                    query = q_buf[q_span, m * head_size : (m + 1) * head_size]
                    keys = k_buf[k_span, m * head_size : (m + 1) * head_size]
                found.append(
                    lax.dot_general(
                        query, keys, (((1,), (1,)), ((), ())), preferred_element_type=jnp.float32
                    )
                )
            for m in range(2):
                scores = found[m]
                if edge is not None:
                    row = lax.broadcasted_iota(jnp.int32, scores.shape, 0)
                    col = lax.broadcasted_iota(jnp.int32, scores.shape, 1)
                    scores = jnp.where(col - row <= edge, scores, NEG_FILL)
                old_peak = peak[m, q_span, :]
                new_peak = jnp.maximum(old_peak, jnp.max(scores, axis=1, keepdims=True) * scale)
                weights = jnp.exp2(scores * scale - jnp.concatenate([new_peak] * (count // 128), axis=1))
                factor = jnp.exp2(old_peak - new_peak)
                partial = weights[:, :128]
                for piece in range(1, count // 128):
                    partial = partial + weights[:, piece * 128 : (piece + 1) * 128]
                read = jnp.dot(weights.astype(jnp.bfloat16), values, preferred_element_type=jnp.float32)
                spread = factor if value_size == 128 else jnp.concatenate([factor] * (value_size // 128), axis=1)
                acc[m, q_span, :value_size] = acc[m, q_span, :value_size] * spread + read
                total[m, q_span, :] = total[m, q_span, :] * factor + partial
                peak[m, q_span, :] = new_peak

        def one_step(step, carry):
            word = sum(jnp.where(step == at, here[at], 0) for at in range(steps))
            i, j = word % 4, word // 4 % 4
            passed = word // 128

            @pl.when(passed > 0)
            def _():
                for what in (1, 2):
                    from_level(kind, what, passed - 1).wait_recv()
                    across(kind, what, passed - 1, False).start()

            @pl.when(word // 16 % 2 == 1)
            def _():
                from_level(kind, 0, i).wait_recv()

            @pl.when(word // 32 % 2 == 1)
            def _():
                for what in (1, 2):
                    from_across(kind, what, j).wait_recv()

            result = kinds[kind]["result"]
            weight = lam[kind, level // 2]

            def tile(at, inner):
                q_at = i * tokens + at * rows

                @pl.when(i != j)
                def _():
                    update(q_at, 2 * j * tokens, 2 * tokens, None)

                @pl.when(i == j)
                def _():
                    @pl.when(side == 1)
                    def _():
                        update(q_at, 2 * i * tokens, tokens, None)

                    @pl.when(at == 0)
                    def _():
                        update(q_at, (2 * i + side) * tokens, rows, 0)

                    @pl.when(at > 0)
                    def _():
                        update(q_at, (2 * i + side) * tokens, tokens, at * rows)

                @pl.when(word // 64 % 2 == 1)
                def _():
                    span = pl.ds(pl.multiple_of(q_at, rows), rows)
                    first, second = (
                        acc[m, span, :value_size] / jnp.sum(total[m, span, :], axis=1, keepdims=True)
                        for m in range(2)
                    )
                    mixed = first - weight * second
                    result[span, :] = (
                        mixed * lax.rsqrt(jnp.mean(mixed * mixed, axis=1, keepdims=True) + 1e-06)
                    ).astype(result.dtype)
                    for near in range(rows // share):
                        part = at * (rows // share) + near
                        mine = jnp.logical_and(i == level, me_tp == part)
                        pl.when(mine)(lambda part=part: keep_result(kind, part).start())
                        pl.when(jnp.logical_not(mine))(lambda part=part: deliver(kind, i, part).start())

                return inner

            lax.fori_loop(0, tokens // rows, tile, 0)
            return carry

        lax.fori_loop(0, steps, one_step, 0)

        for what in (1, 2):
            for at in range(levels):
                pl.when(level == at)(lambda what=what, at=at: across(kind, what, at, True).wait_send())
                pl.when(level != at)(lambda what=what, at=at: across(kind, what, at, False).wait_send())
        for i in range(levels):
            for part in range(tp_count):
                mine = jnp.logical_and(i == level, me_tp == part)
                pl.when(mine)(lambda part=part: keep_result(kind, part).wait())
                pl.when(jnp.logical_not(mine))(lambda i=i, part=part: deliver(kind, i, part).wait_send())

    groups = 2 * levels
    slots = outgoing.shape[0] // groups
    route(ids, shares, place, notes, groups, slots)

    of_kind(level, run)

    for which in range(2):
        share_shard(which, 1, peer, peer, False).wait_recv()
        shard_copy(which, 2).start()

    for rising, valid, one in over_targets((0, 1, 2), lambda copy: copy.wait_send()):
        pl.when(valid)(one)
    for origin in range(levels):
        for part in range(tp_count):
            kind = (origin + part) % 2
            ref = kinds[kind]["out"].at[:, column(kind, origin, part)]

            @pl.when(jnp.logical_not(jnp.logical_and(origin == level, part == me_tp)))
            def _(origin=origin, part=part, ref=ref):
                pltpu.make_async_remote_copy(
                    src_ref=ref, dst_ref=ref, send_sem=o_send.at[origin, part],
                    recv_sem=o_recv.at[origin, part], device_id=(2 * origin + side, part),
                    device_id_type=MESH,
                ).wait_recv()

    for which in range(2):
        keep_shard(which).wait()
        for at in range(3):
            shard_copy(which, at).wait_send()
        share_shard(which, 0, sibling, sibling, False).wait_recv()
        share_shard(which, 2, sibling, 2 * (1 - tp_y) + 1 - tp_core, False).wait_recv()

    width = stream.shape[1]
    step = math.gcd(width, 512)
    squares = jnp.zeros((share, 128), jnp.float32)

    def project(at, squares):
        span = pl.ds(pl.multiple_of(at * step, step), step)
        summed = jnp.dot(wide_out[...], pw[:, span], preferred_element_type=jnp.float32)
        summed = summed + jnp.dot(narrow_out[...], pn[:, span], preferred_element_type=jnp.float32)
        rounded = (summed + residual[:, span].astype(jnp.float32)).astype(stream.dtype)
        stream[:, span] = rounded
        value = rounded.astype(jnp.float32)
        square = value * value
        for piece in range(step // 128):
            squares = squares + square[:, piece * 128 : (piece + 1) * 128]
        return squares

    squares = lax.fori_loop(0, width // step, project, squares)
    factor = lax.rsqrt(jnp.sum(squares, axis=1, keepdims=True) / width + 1e-06)

    def normalize(at, carry):
        span = pl.ds(pl.multiple_of(at * step, step), step)
        normed[:, span] = (stream[:, span].astype(jnp.float32) * factor * gain[:, span]).astype(
            normed.dtype
        )
        return carry

    lax.fori_loop(0, width // step, normalize, 0)

    def dispatch(at, carry):
        span = pl.ds(pl.multiple_of(at * step, step), step)
        outgoing[:, span] = jnp.dot(
            place[...], normed[:, span], preferred_element_type=jnp.float32
        ).astype(outgoing.dtype)
        return carry

    lax.fori_loop(0, width // step, dispatch, 0)
    outgoing[:, width:] = lax.dot_general(
        place[...], notes[...], (((1,), (1,)), ((), ())), preferred_element_type=jnp.float32
    ).astype(outgoing.dtype)


def exchange_attention(
    lam, qw, kw, vw, qn, kn, vn, pw, pn, residual, gain, ids, shares, levels, tp_count, heads, slots
):
    tokens = qw.shape[0]
    share = tokens // tp_count
    wide, narrow = [x.shape[1] // heads for x in (qw, kw, vw)], [x.shape[1] // heads for x in (qn, kn, vn)]
    most = max(wide[2], narrow[2])
    rows = levels * tokens

    def buffers(widths):
        return [
            pltpu.VMEM((rows, widths[0]), jnp.bfloat16),
            pltpu.VMEM((2 * rows, widths[1]), jnp.bfloat16),
            pltpu.VMEM((2 * rows, widths[2]), jnp.bfloat16),
        ]

    pairs = 2 * rows * rows * 2
    return pl.pallas_call(
        functools.partial(exchange_kernel, levels=levels, tp_count=tp_count, heads=heads),
        in_specs=[pl.BlockSpec(memory_space=pltpu.SMEM)] + [pl.BlockSpec(memory_space=pl.ANY)] * 8
        + [pl.BlockSpec(memory_space=pltpu.VMEM)] * 4,
        out_specs=[pl.BlockSpec(memory_space=pltpu.VMEM)] * 3,
        out_shape=[
            jax.ShapeDtypeStruct(residual.shape, jnp.bfloat16),
            jax.ShapeDtypeStruct((2 * levels * slots, residual.shape[1] + 128), jnp.bfloat16),
            jax.ShapeDtypeStruct((2 * levels * slots, share), jnp.bfloat16),
        ],
        scratch_shapes=buffers(wide)
        + buffers(narrow)
        + [
            pltpu.VMEM((2, rows, most), jnp.float32),
            pltpu.VMEM((2, rows, 128), jnp.float32),
            pltpu.VMEM((2, rows, 128), jnp.float32),
            pltpu.VMEM((rows, wide[2]), jnp.bfloat16),
            pltpu.VMEM((rows, narrow[2]), jnp.bfloat16),
            pltpu.VMEM((share, tp_count * heads * wide[2]), jnp.bfloat16),
            pltpu.VMEM((share, tp_count * heads * narrow[2]), jnp.bfloat16),
            pltpu.VMEM((tp_count * pw.shape[0], pw.shape[1]), jnp.bfloat16),
            pltpu.VMEM((tp_count * pn.shape[0], pn.shape[1]), jnp.bfloat16),
            pltpu.VMEM(residual.shape, jnp.bfloat16),
            pltpu.VMEM((128, share), jnp.bfloat16),
            pltpu.SemaphoreType.DMA((6,)),
            pltpu.SemaphoreType.DMA((3, levels)),
            pltpu.SemaphoreType.DMA((3, levels)),
            pltpu.SemaphoreType.DMA((3, levels)),
            pltpu.SemaphoreType.DMA((3, levels)),
            pltpu.SemaphoreType.DMA((levels, tp_count)),
            pltpu.SemaphoreType.DMA((levels, tp_count)),
            pltpu.SemaphoreType.DMA((2, 3)),
            pltpu.SemaphoreType.DMA((2, 3)),
        ],
        compiler_params=pltpu.CompilerParams(
            vmem_limit_bytes=58 * 1024 * 1024, has_side_effects=True
        ),
        cost_estimate=pl.CostEstimate(
            flops=pairs * 1024, bytes_accessed=tokens * 4096 * 8, transcendentals=pairs
        ),
    )(lam, qw, kw, vw, qn, kn, vn, pw, pn, residual, gain, ids, shares)


def level_orders(levels):
    return [
        sorted(range(levels), key=lambda other: (abs(other - level), -other)) for level in range(levels)
    ]


def expert_kernel(
    outgoing, gate_in, up_in, down_in, returned,
    rows, gate, up, down, chosen, hidden, result, part, got_one, sum_one, got_two, final,
    own_sem, z_send, z_recv, y_send, y_recv, s_send, s_recv,
    one_send, one_recv, two_send, two_recv, back_send, back_recv,
    *, levels, slots, capacity,
):
    me_sp, me_tp = lax.axis_index("sp"), lax.axis_index("tp")
    level, side = me_sp // 2, me_sp % 2
    tp_y, tp_core = me_tp // 2, me_tp % 2
    sibling, peer = 2 * tp_y + 1 - tp_core, 2 * (1 - tp_y) + tp_core
    corner = 2 * (1 - tp_y) + 1 - tp_core
    width = returned.shape[1]
    group_rows, picked = GROUP * slots, GROUP * capacity
    orders = level_orders(levels)

    def pick_level(turn):
        return sum(
            jnp.where(jnp.logical_and(level == at, turn == place), orders[at][place], 0)
            for at in range(levels)
            for place in range(levels)
        )

    def span(index, size):
        return pl.ds(pl.multiple_of(index * size, size), size)

    def block(ref, origin, at_tp):
        return ref.at[span(origin * GROUP + at_tp, slots), :]

    def send(src, dst, send_sem, recv_sem, target):
        return pltpu.make_async_remote_copy(
            src_ref=src, dst_ref=dst, send_sem=send_sem, recv_sem=recv_sem,
            device_id=target, device_id_type=MESH,
        )

    def out_copy(target):
        return send(
            outgoing.at[span(target, slots), :], block(rows, me_sp, me_tp),
            z_send.at[target], z_recv.at[me_sp], (target, me_tp),
        )

    def out_keep():
        return pltpu.make_async_copy(
            outgoing.at[span(me_sp, slots), :], block(rows, me_sp, me_tp), own_sem.at[0]
        )

    def arrival(ref, sem, target):
        return send(ref, ref, z_send.at[0], sem, target)

    def y_copy(origin):
        ref = block(rows, origin, me_tp)
        return send(ref, ref, y_send.at[origin], y_recv.at[origin], (me_sp, peer))

    def s_copy(origin, which):
        ref = block(rows, origin, peer if which else me_tp)
        return send(ref, ref, s_send.at[origin, which], s_recv.at[origin, which], (me_sp, sibling))

    def one_copy(origin, half):
        return send(
            block(part, origin, 2 * half + 1 - tp_core), got_one.at[span(2 * origin + half, slots), :],
            one_send.at[origin, half], one_recv.at[origin, half], (me_sp, sibling),
        )

    def two_copy(origin):
        return send(
            sum_one.at[span(origin, slots), :], got_two.at[span(origin, slots), :],
            two_send.at[origin], two_recv.at[origin], (me_sp, peer),
        )

    def back_copy(origin):
        return send(
            final.at[span(origin, slots), :], returned.at[span(me_sp, slots), :],
            back_send.at[origin], back_recv.at[me_sp], (origin, me_tp),
        )

    weights = [
        pltpu.make_async_copy(src, dst, own_sem.at[1 + at])
        for at, (src, dst) in enumerate(((gate_in, gate), (up_in, up), (down_in, down)))
    ]
    out_keep().start()
    for turn in range(levels):
        there = pick_level(turn)
        for other in range(2):
            if turn == 0 and other == 0:
                continue
            out_copy(2 * there + (side + other) % 2).start()
    for copy in weights:
        copy.start()

    def both(turn, body):
        there = pick_level(turn)
        for other in range(2):
            body(2 * there + (side + other) % 2, other)

    def spread(origin, other):
        pl.when(origin == me_sp)(lambda: out_keep().wait())
        pl.when(origin != me_sp)(
            lambda: arrival(block(rows, origin, me_tp), z_recv.at[origin], (me_sp, peer)).wait_recv()
        )
        y_copy(origin).start()
        s_copy(origin, 0).start()

    def pass_on(origin, other):
        arrival(block(rows, origin, peer), y_recv.at[origin], (me_sp, peer)).wait_recv()
        s_copy(origin, 1).start()

    def selection(origin):
        notes = rows[span(origin, group_rows), width:].astype(jnp.float32)
        lane = lax.broadcasted_iota(jnp.int32, notes.shape, 1)
        rank = jnp.sum(jnp.where(lane == me_tp, notes, 0.0), axis=1, keepdims=True)
        share = jnp.sum(
            jnp.where(jnp.logical_and(lane >= GROUP, lane % GROUP == me_tp), notes, 0.0),
            axis=1, keepdims=True,
        )
        at_row = lax.broadcasted_iota(jnp.int32, (group_rows, picked), 0)
        at_col = lax.broadcasted_iota(jnp.int32, (group_rows, picked), 1)
        wanted = (at_col - at_row // slots * capacity + 1).astype(jnp.float32)
        hit = jnp.logical_and(wanted == rank, rank > 0.5)
        return hit.astype(jnp.float32).astype(jnp.bfloat16), share

    def choose(origin, other):
        arrival(block(rows, origin, sibling), s_recv.at[origin, 0], (me_sp, sibling)).wait_recv()
        arrival(block(rows, origin, corner), s_recv.at[origin, 1], (me_sp, sibling)).wait_recv()
        table, _ = selection(origin)
        chosen[other * picked : (other + 1) * picked, :] = lax.dot_general(
            table, rows[span(origin, group_rows), :width], (((0,), (0,)), ((), ())),
            preferred_element_type=jnp.float32,
        ).astype(jnp.bfloat16)

    def experts():
        tile = math.gcd(hidden.shape[1], 256)

        def inner(at, carry):
            cols = span(at, tile)
            gated = jnp.dot(chosen[...], gate[:, cols], preferred_element_type=jnp.float32)
            lifted = jnp.dot(chosen[...], up[:, cols], preferred_element_type=jnp.float32)
            hidden[:, cols] = (gated / (1.0 + jnp.exp(-gated)) * lifted).astype(jnp.bfloat16)
            return carry

        lax.fori_loop(0, hidden.shape[1] // tile, inner, 0)
        wide = math.gcd(width, 512)

        def outer(at, carry):
            cols = span(at, wide)
            result[:, cols] = jnp.dot(
                hidden[...], down[:, cols], preferred_element_type=jnp.float32
            ).astype(jnp.bfloat16)
            return carry

        lax.fori_loop(0, width // wide, outer, 0)

    def spread_result(origin, other):
        table, share = selection(origin)
        wide = math.gcd(width, 512)
        for at in range(width // wide):
            cols = slice(at * wide, (at + 1) * wide)
            placed = jnp.dot(
                table, result[other * picked : (other + 1) * picked, cols],
                preferred_element_type=jnp.float32,
            )
            part[span(origin, group_rows), cols] = (share * placed).astype(jnp.bfloat16)
        for half in range(2):
            one_copy(origin, half).start()

    def add_one(origin, other):
        for half in range(2):
            arrival(
                got_one.at[span(2 * origin + half, slots), :], one_recv.at[origin, half], (me_sp, sibling)
            ).wait_recv()
        away = 1 - tp_y
        mine = part[span(origin * GROUP + 2 * away + tp_core, slots), :].astype(jnp.float32)
        theirs = got_one[span(2 * origin + away, slots), :].astype(jnp.float32)
        sum_one[span(origin, slots), :] = (mine + theirs).astype(jnp.bfloat16)
        two_copy(origin).start()

    def add_two(origin, other):
        arrival(got_two.at[span(origin, slots), :], two_recv.at[origin], (me_sp, peer)).wait_recv()
        mine = part[span(origin * GROUP + me_tp, slots), :].astype(jnp.float32)
        theirs = got_one[span(2 * origin + tp_y, slots), :].astype(jnp.float32)
        summed = mine + theirs + got_two[span(origin, slots), :].astype(jnp.float32)
        final[span(origin, slots), :] = summed.astype(jnp.bfloat16)
        pl.when(origin != me_sp)(lambda: back_copy(origin).start())

        @pl.when(origin == me_sp)
        def _():
            returned[span(me_sp, slots), :] = summed.astype(jnp.bfloat16)

    def turn_body(turn, carry):
        @pl.when(turn == 1)
        def _():
            for copy in weights:
                copy.wait()

        @pl.when(turn < levels)
        def _():
            both(turn, spread)

        @pl.when(jnp.logical_and(turn >= 1, turn < levels + 1))
        def _():
            both(turn - 1, pass_on)

        @pl.when(turn >= 2)
        def _():
            both(turn - 2, add_two)

        @pl.when(jnp.logical_and(turn >= 1, turn < levels + 1))
        def _():
            both(turn - 1, choose)
            experts()
            both(turn - 1, spread_result)

        @pl.when(jnp.logical_and(turn >= 1, turn < levels + 1))
        def _():
            both(turn - 1, add_one)

        return carry

    lax.fori_loop(0, levels + 2, turn_body, 0)

    def drain(origin, carry):
        @pl.when(origin != me_sp)
        def _():
            out_copy(origin).wait_send()
            back_copy(origin).wait_send()
            arrival(
                returned.at[span(origin, slots), :], back_recv.at[origin], (origin, me_tp)
            ).wait_recv()

        y_copy(origin).wait_send()
        two_copy(origin).wait_send()
        for which in range(2):
            s_copy(origin, which).wait_send()
            one_copy(origin, which).wait_send()
        return carry

    lax.fori_loop(0, 2 * levels, drain, 0)


def grouped_experts(stream, outgoing, place, gate, up, down, sp_size, slots, capacity):
    width = stream.shape[1]
    levels = sp_size // 2
    every = sp_size * GROUP * slots
    own = sp_size * slots
    picked = 2 * GROUP * capacity
    hidden_size = gate.shape[1]
    dma = pltpu.SemaphoreType.DMA
    returned = pl.pallas_call(
        functools.partial(expert_kernel, levels=levels, slots=slots, capacity=capacity),
        in_specs=[pl.BlockSpec(memory_space=pl.ANY)] * 4,
        out_specs=pl.BlockSpec(memory_space=pltpu.VMEM),
        out_shape=jax.ShapeDtypeStruct((own, width), jnp.bfloat16),
        scratch_shapes=[
            pltpu.VMEM((every, outgoing.shape[1]), jnp.bfloat16),
            pltpu.VMEM(gate.shape, jnp.bfloat16),
            pltpu.VMEM(up.shape, jnp.bfloat16),
            pltpu.VMEM(down.shape, jnp.bfloat16),
            pltpu.VMEM((picked, width), jnp.bfloat16),
            pltpu.VMEM((picked, hidden_size), jnp.bfloat16),
            pltpu.VMEM((picked, width), jnp.bfloat16),
            pltpu.VMEM((every, width), jnp.bfloat16),
            pltpu.VMEM((2 * own, width), jnp.bfloat16),
            pltpu.VMEM((own, width), jnp.bfloat16),
            pltpu.VMEM((own, width), jnp.bfloat16),
            pltpu.VMEM((own, width), jnp.bfloat16),
            dma((4,)),
        ]
        + [dma((sp_size,))] * 4
        + [dma((sp_size, 2))] * 4
        + [dma((sp_size,))] * 4,
        compiler_params=pltpu.CompilerParams(
            vmem_limit_bytes=58 * 1024 * 1024, has_side_effects=True
        ),
        cost_estimate=pl.CostEstimate(
            flops=6 * own * width * hidden_size * 2,
            bytes_accessed=6 * width * hidden_size,
            transcendentals=own * hidden_size,
        ),
    )(outgoing, gate, up, down)
    summed = lax.dot_general(
        place, returned, (((0,), (0,)), ((), ())), preferred_element_type=jnp.float32
    )
    return (stream.astype(jnp.float32) + summed).astype(jnp.bfloat16)


def ring_order(count):
    return list(range(0, count, 2)) + list(range(1, count, 2))[::-1]


def ring_attention(
    query_wide, key_wide, value_wide, query_narrow, key_narrow, value_narrow, mix_lambda
):
    tok_count, local_heads, _ = query_wide.shape
    size_wide = query_wide.shape[2] // 2
    size_narrow = query_narrow.shape[2] // 2

    value_wide_size, value_narrow_size = value_wide.shape[2], value_narrow.shape[2]
    flat = lambda member: member.reshape(tok_count, -1)
    own = jnp.concatenate(
        [flat(key_wide), flat(value_wide), flat(key_narrow), flat(value_narrow)], axis=1
    )
    wide_q, narrow_q = flat(query_wide), flat(query_narrow)
    wide_v_col = local_heads * 2 * size_wide
    narrow_k_col = wide_v_col + local_heads * value_wide_size
    narrow_v_col = narrow_k_col + local_heads * 2 * size_narrow

    count = lax.axis_size("sp")
    order = ring_order(count)
    place = [order.index(device) for device in range(count)]
    me = lax.axis_index("sp")
    order_table = jnp.array(order, jnp.int32)
    my_place = jnp.array(place, jnp.int32)[me]
    forward = [(order[i], order[(i + 1) % count]) for i in range(count)]
    backward = [(b, a) for a, b in forward]

    def source_flag(shift):
        return (order_table[(my_place + shift) % count] < me).astype(jnp.int32)

    def both(pieces, flags, states, final=False):
        return (
            attend(
                wide_q, pieces, flags, states[0], mix_lambda[0], size_wide, value_wide_size,
                0, wide_v_col, final,
            ),
            attend(
                narrow_q, pieces, flags, states[1], mix_lambda[1], size_narrow, value_narrow_size,
                narrow_k_col, narrow_v_col, final,
            ),
        )

    half = tok_count // 2
    pieces = [(own, 0, tok_count)]
    flags = jnp.ones((2,), jnp.int32)
    states = (None, None)
    left = right = own
    for step in range(1, count // 2 + 1):
        if step < count // 2:
            left = lax.ppermute(left, "sp", forward)
            right = lax.ppermute(right, "sp", backward)
            coming = [(left, 0, tok_count), (right, 0, tok_count)]
        else:
            coming = [
                (lax.ppermute(left[:half], "sp", forward), 0, half),
                (lax.ppermute(right[half:], "sp", backward), 0, half),
            ]
        states = both(pieces, flags, states)
        arrived_now, states = lax.optimization_barrier(
            (tuple(piece for piece, _, _ in coming), states)
        )
        pieces = [(arrived_now[i], 0, coming[i][2]) for i in range(2)]
        left, right = arrived_now
        flags = jnp.stack([source_flag(-step), source_flag(step)])
    heads_wide, heads_narrow = both(pieces, flags, states, final=True)
    return (
        lax.all_to_all(heads_wide, "tp", split_axis=0, concat_axis=1, tiled=True),
        lax.all_to_all(heads_narrow, "tp", split_axis=0, concat_axis=1, tiled=True),
    )


def shards(
    query_wide,
    key_wide,
    value_wide,
    query_narrow,
    key_narrow,
    value_narrow,
    mix_lambda,
    residual_in,
    out_wide,
    out_narrow,
    ffn_gain,
    expert_ids,
    expert_weights,
    gate_weight,
    up_weight,
    down_weight,
):
    tok_count, local_heads, _ = query_wide.shape
    tp_size, sp_size = lax.axis_size("tp"), lax.axis_size("sp")
    local_rows = tok_count // tp_size
    attention_args = (
        query_wide, key_wide, value_wide, query_narrow, key_narrow, value_narrow, mix_lambda
    )
    fits = sp_size == 8 and local_heads * 4 == sp_size and tp_size == GROUP
    if fits:
        flat = [member.reshape(tok_count, -1) for member in attention_args[:6]]
        capacity = max(2, 4 * local_rows // (sp_size * tp_size))
        slots = GROUP * capacity // 2
        stream, outgoing, place = exchange_attention(
            mix_lambda, *flat, out_wide, out_narrow, residual_in, ffn_gain[None, :],
            expert_ids.T, expert_weights.T, sp_size // 2, tp_size, local_heads, slots,
        )
        return grouped_experts(
            stream, outgoing, place, gate_weight[0], up_weight[0], down_weight[0],
            sp_size, slots, capacity,
        )
    mine_wide, mine_narrow = ring_attention(*attention_args)
    whole_wide, whole_narrow = (
        lax.all_gather(out_wide, "tp", axis=0, tiled=True),
        lax.all_gather(out_narrow, "tp", axis=0, tiled=True),
    )
    projected = jnp.dot(mine_wide, whole_wide, preferred_element_type=jnp.float32) + jnp.dot(
        mine_narrow, whole_narrow, preferred_element_type=jnp.float32
    )
    stream = (projected + residual_in.astype(jnp.float32)).astype(jnp.bfloat16)
    stream_f = stream.astype(jnp.float32)
    normed = (
        stream_f
        * lax.rsqrt(jnp.mean(stream_f * stream_f, axis=-1, keepdims=True) + 1e-06)
        * ffn_gain
    ).astype(jnp.bfloat16)
    experts_all = lax.axis_size("sp") * tp_size
    capacity = max(2, 4 * local_rows // experts_all)
    model_width = normed.shape[1]
    flat_expert = expert_ids.reshape(-1)
    expert_hot = (flat_expert[:, None] == jnp.arange(experts_all, dtype=jnp.int32)[None, :]).astype(
        jnp.int32
    )
    slot_rank = jnp.sum((jnp.cumsum(expert_hot, axis=0) - 1) * expert_hot, axis=1)
    flat_slot = flat_expert * capacity + slot_rank
    slot_ids = jnp.arange(experts_all * capacity, dtype=jnp.int32)
    placed = slot_ids[:, None] == flat_slot[None, :]
    dispatch = jnp.any(placed.reshape(experts_all * capacity, local_rows, 2), axis=2).astype(
        jnp.bfloat16
    )
    outgoing = jnp.dot(dispatch, normed, preferred_element_type=jnp.float32).astype(jnp.bfloat16)
    outgoing = outgoing.reshape(experts_all, capacity, model_width)
    arrived = lax.all_to_all(outgoing, ("sp", "tp"), split_axis=0, concat_axis=0, tiled=True)
    sources, items, width = arrived.shape
    flat_rows = arrived.reshape(sources * items, width)
    gate_part = jnp.dot(flat_rows, gate_weight[0], preferred_element_type=jnp.float32)
    up_part = jnp.dot(flat_rows, up_weight[0], preferred_element_type=jnp.float32)
    hidden = (jax.nn.silu(gate_part) * up_part).astype(jnp.bfloat16)
    result = jnp.dot(hidden, down_weight[0], preferred_element_type=jnp.float32).astype(
        jnp.bfloat16
    )
    returned = lax.all_to_all(
        result.reshape(sources, items, width), ("sp", "tp"), split_axis=0, concat_axis=0, tiled=True
    )
    slot_hot = (flat_slot[:, None] == slot_ids[None, :]).astype(
        jnp.float32
    ) * expert_weights.reshape(-1)[:, None]
    combine = jnp.sum(slot_hot.reshape(local_rows, 2, experts_all * capacity), axis=1)
    summed = jnp.dot(
        combine,
        returned.reshape(experts_all * capacity, model_width).astype(jnp.float32),
        precision=lax.Precision.HIGHEST,
    )
    return (stream_f + summed).astype(jnp.bfloat16)


def solution(mesh):
    return jax.shard_map(
        shards,
        mesh=mesh,
        in_specs=(
            P("sp", "tp", None),
            P("sp", "tp", None),
            P("sp", "tp", None),
            P("sp", "tp", None),
            P("sp", "tp", None),
            P("sp", "tp", None),
            P(None, "tp"),
            P(("sp", "tp"), None),
            P("tp", None),
            P("tp", None),
            P(),
            P(("sp", "tp"), None),
            P(("sp", "tp"), None),
            P(("sp", "tp"), None, None),
            P(("sp", "tp"), None, None),
            P(("sp", "tp"), None, None),
        ),
        out_specs=P(("sp", "tp"), None),
        check_vma=False,
    )
```
